32 devices in a mesh: grp: 2 (over y), sp: 4 (over z), tp: 4 (over x, core).
Axes of the slice: x: 2, y: 2, z: 4, core: 2. Of those that a mesh axis runs over, the one named last changes fastest.
Arguments:
- target: bfloat16 [1024, 2048], P(('grp', 'sp', 'tp')), parts along dimension 0, may hold values from -60 to 60
- source: bfloat16 [8192, 2048], P(('grp', 'sp', 'tp')), parts along dimension 0, may hold values from -120 to 120
- w_query: bfloat16 [2, 2048, 2048], P(None, None, 'tp'), may hold values from -0.176776695 to 0.176776695
- w_key: bfloat16 [2, 2048, 2048], P(None, None, 'tp'), may hold values from -0.176776695 to 0.176776695
- w_value: bfloat16 [2, 2048, 2048], P(None, None, 'tp'), may hold values from -0.125 to 0.125
- w_out: bfloat16 [2, 2048, 2048], P(None, 'tp'), may hold values from -0.125 to 0.125
- gains: float32 [2, 2, 2048], replicated, may hold values from 0.1 to 1.9
Outputs:
- mixed: bfloat16 [1024, 2048], P(('grp', 'sp', 'tp')), parts along dimension 0
The draws below stay inside these ranges and needn't reach their ends.
There are 2 independent parts, one for each index of `grp`. The reference program is written for one: setup_inputs(seed, part) draws one part's arguments, and reference() takes and returns one part's arrays. A program takes and returns all parts, laid end to end along the dimension named above; an argument that names none is the same for every part. Nothing has to cross between parts.
All inputs are finite; a program needn't handle non-finite values.
Results may differ from the reference program's by a relative error of at most 0.025.
Values may be sent and summed in bfloat16 or wider, within the bound.
A program may use at most 128 MiB of HBM per device.

```python
import jax
import jax.numpy as jnp
from jax import lax

D = 2048
HEADS = 16
HEAD = 128
LAYERS = 2
TGT = 512
SRC = 4096
N_TP = 4


def draw_target(key, part):
    base = jnp.clip(jax.random.normal(jax.random.fold_in(key, 11), (TGT, D), jnp.float32), -6.0, 6.0)
    return base.astype(jnp.bfloat16)


def draw_source(key, part):
    base = jnp.clip(jax.random.normal(jax.random.fold_in(key, 21), (SRC, D), jnp.float32), -6.0, 6.0)
    return base.astype(jnp.bfloat16)


def draw_w_query(key, part):
    shared = jnp.clip(jax.random.normal(jax.random.fold_in(key, 31), (LAYERS, D, D), jnp.float32), -6.0, 6.0)
    return (shared * D ** (-0.5)).astype(jnp.bfloat16)


def draw_w_key(key, part):
    fresh = jnp.clip(jax.random.normal(jax.random.fold_in(key, 32), (LAYERS, D, D), jnp.float32), -6.0, 6.0)
    return (fresh * D ** (-0.5)).astype(jnp.bfloat16)


def steps_of(key, extent, pieces, smallest, top_value):
    level = 1.0
    for dim, shards_of in pieces:
        steps = jax.random.uniform(jax.random.fold_in(jax.random.fold_in(key, 6), dim), (shards_of,), jnp.float32, smallest / len(pieces), top_value / len(pieces))
        level = level * jnp.repeat(jnp.exp(steps), extent[dim] // shards_of).reshape((-1,) + (1,) * (len(extent) - 1 - dim))
    return level


def bell_draw(rng, extent, width, bound, cuts=(), held_as=jnp.bfloat16):
    result = jax.random.normal(rng, extent, jnp.float32) * width
    if len(cuts) > 0:
        result = steps_of(rng, extent, cuts, -0.22, 0.18) * result
    return jnp.clip(result, min=-bound, max=bound).astype(held_as)


def setup_inputs(seed: int = 0, part: int = 0) -> dict:
    key_list = jax.random.split(jax.random.key(seed), 8)
    part_splits = jax.random.split(jax.random.fold_in(key_list[7], part), 8)
    return {
        "target": draw_target(jax.random.fold_in(jax.random.fold_in(key_list[7], part), 71), part),
        "source": draw_source(jax.random.fold_in(jax.random.fold_in(key_list[7], part), 71), part),
        "w_query": draw_w_query(jax.random.fold_in(key_list[7], 71), part),
        "w_key": draw_w_key(jax.random.fold_in(key_list[7], 71), part),
        "w_value": bell_draw(key_list[4], (LAYERS, D, D), D ** -0.5, 0.125, ((2, 4),)),
        "w_out": bell_draw(key_list[5], (LAYERS, D, D), D ** -0.5, 0.125, ((1, 4),)),
        "gains": jnp.clip(1.0 + 0.18 * jax.random.normal(key_list[6], (LAYERS, 2, D), jnp.float32), 0.1, 1.9),
    }


EPS = 1e-06

def normalize(row_block, gain_row):
    return row_block * lax.rsqrt(lax.optimization_barrier(jnp.mean(row_block * row_block, axis=-1, keepdims=True)) + EPS) * gain_row.astype(jnp.float32)

def attend_head(query_cols, key_cols, value_cols):
    scores = jnp.dot(query_cols, key_cols.T, preferred_element_type=jnp.float32) * HEAD ** (-0.5)
    row_peak = lax.optimization_barrier(jnp.max(scores, axis=1, keepdims=True))
    weights = jnp.exp(scores - row_peak)
    row_total = lax.optimization_barrier(jnp.sum(weights, axis=1, keepdims=True))
    summed = jnp.dot(weights.astype(jnp.bfloat16), value_cols, preferred_element_type=jnp.float32)
    return (summed / row_total).astype(jnp.bfloat16)

def reference(target, source, w_query, w_key, w_value, w_out, gains):
    stream = target.astype(jnp.float32)
    group_width = D // N_TP
    for layer_index in range(LAYERS):
        keys = jnp.dot(source, w_key[layer_index], preferred_element_type=jnp.float32).astype(jnp.bfloat16)
        values = jnp.dot(source, w_value[layer_index], preferred_element_type=jnp.float32).astype(jnp.bfloat16)
        normed = normalize(stream, gains[layer_index, 0]).astype(jnp.bfloat16)
        queries = jnp.dot(normed, w_query[layer_index], preferred_element_type=jnp.float32).astype(jnp.bfloat16)

        def one_head(head_index):
            offset = (head_index * HEAD).astype(jnp.int32)
            return attend_head(lax.dynamic_slice_in_dim(queries, offset, HEAD, 1), lax.dynamic_slice_in_dim(keys, offset, HEAD, 1), lax.dynamic_slice_in_dim(values, offset, HEAD, 1))
        heads_out = lax.map(one_head, jnp.arange(HEADS, dtype=jnp.int32))
        attended = jnp.transpose(heads_out, (1, 0, 2)).reshape(TGT, D)
        out_weight = w_out[layer_index]

        def add_group(running, group_index):
            offset = (group_index * group_width).astype(jnp.int32)
            partial_value = jnp.dot(lax.dynamic_slice_in_dim(attended, offset, group_width, 1), lax.dynamic_slice_in_dim(out_weight, offset, group_width, 0), preferred_element_type=jnp.float32)
            rounded = lax.optimization_barrier(partial_value.astype(jnp.bfloat16))
            return (running + rounded.astype(jnp.float32), None)
        projected, _ = lax.scan(add_group, jnp.zeros((TGT, D), jnp.float32), jnp.arange(N_TP, dtype=jnp.int32))
        stream = stream + normalize(projected, gains[layer_index, 1])
    return stream.astype(jnp.bfloat16)
```

```python
import functools
import math

import jax
import jax.numpy as jnp
from jax import lax
from jax.experimental import pallas as pl
from jax.experimental.pallas import tpu as pltpu
from jax.sharding import PartitionSpec as P

HEAD = 128
CORES = 2
PIECES = 2


EPS = 1e-06
MESH = pl.DeviceIdType.MESH
F32 = jnp.float32
LOWEST = -1e30
BF16 = jnp.bfloat16


def normalize(row_block, gain_row):
    return (
        row_block
        * lax.rsqrt(jnp.mean(row_block * row_block, axis=-1, keepdims=True) + EPS)
        * gain_row
    )


def fused_kernel(
    nx, sp, depth,
    target, source, w_query, w_key, w_value, w_out, gains, out,
    tbuf, sbuf, wq, wk, wv, wo, keys, values, stream, normed, qbuf,
    osend, orecv, ssend, srecv, orelay, srelay, attended, pbuf, half_in, chip_sum, fin,
    local_sem, weight_sem, t_send, t_recv, t_fsend, s_psend, s_send, s_recv, s_fsend,
    q_send, q_recv, q_fsend, o_send, o_recv, e_send, e_recv, or_recv, er_recv,
    h_send, h_recv, c_send, c_psend, c_fsend, c_recv, c_frecv, f_send, f_recv,
):
    s = lax.axis_index("sp")
    t = lax.axis_index("tp")
    x = t // CORES
    c = t % CORES
    partner_c = 1 - c
    partner = {"tp": x * CORES + partner_c}
    units = sbuf.shape[0]
    half = sbuf.shape[2]
    width = sbuf.shape[3]
    rows = 2 * half
    local_width = wk.shape[2]
    heads = local_width // HEAD
    tp = nx * CORES
    prows = stream.shape[2]
    piece_rows = tp * prows
    score_scale = HEAD ** (-0.5) * math.log2(math.e)

    pairs = sp // 2
    edge = jnp.logical_or(s == 0, s == sp - 1)
    mirror = sp - 1 - s
    relays = jnp.logical_or(s == 1, s == sp - 2)
    relay_from = jnp.where(s == 1, 0, sp - 1)
    relay_to = sp - 1 - relay_from
    via = jnp.where(s == 0, 1, sp - 2)

    def chip(step):
        return lax.rem(x + step, nx)

    def peer(step):
        return {"tp": chip(step) * CORES + c}

    def remote(src, dst, send_sem, recv_sem, device):
        return pltpu.make_async_remote_copy(
            src_ref=src, dst_ref=dst, send_sem=send_sem, recv_sem=recv_sem,
            device_id=device, device_id_type=MESH,
        )

    def arrived(dst, recv_sem):
        remote(dst, dst, t_send.at[0], recv_sem, partner).wait_recv()

    own_target = pltpu.make_async_copy(target, tbuf.at[t], local_sem.at[0])
    own_source = [
        pltpu.make_async_copy(
            source.at[pl.ds(part * half, half)], sbuf.at[0, part], local_sem.at[1 + part])
        for part in range(2)
    ]

    def load(kind, level):
        pair = ((w_query, wq), (w_key, wk), (w_value, wv), (w_out, wo))[kind]
        return pltpu.make_async_copy(
            pair[0].at[level], pair[1].at[level], weight_sem.at[kind, level])

    own_target.start()
    for copy in own_source:
        copy.start()
    load(1, 0).start()
    load(2, 0).start()

    barrier = pltpu.get_barrier_semaphore()
    pl.semaphore_signal(barrier, inc=1, device_id=partner, device_id_type=MESH)
    for step in range(1, nx):
        pl.semaphore_signal(barrier, inc=1, device_id=peer(step), device_id_type=MESH)
    for step in range(1, sp):
        pl.semaphore_signal(
            barrier, inc=1, device_id={"sp": lax.rem(s + step, sp)}, device_id_type=MESH)
    with jax.named_scope("barrier"):
        pl.semaphore_wait(barrier, 1 + (nx - 1) + (sp - 1))

    sends = []

    drains = []

    def finish():
        for drain in drains:
            drain()
        for copy in sends:
            copy.wait_send()

    def go(copy):
        copy.start()
        sends.append(copy)

    for step in range(1, nx):
        go(remote(target, tbuf.at[t], t_send.at[step], t_recv.at[t], peer(step)))
    go(remote(target, tbuf.at[t], t_send.at[0], t_recv.at[t], partner))
    for part in range(2):
        block = source.at[pl.ds(part * half, half)]
        for piece in range(2):
            span = pl.ds(piece * (half // 2), half // 2)
            for step in range(1, nx):
                unit = 2 * (nx - step) + part
                go(remote(block.at[span], sbuf.at[unit, 0, span], s_send.at[step, 2 * part + piece],
                          s_recv.at[unit, piece], peer(step)))
        go(remote(block, sbuf.at[1, part], s_psend.at[part], s_recv.at[1, part], partner))

    def project(index):
        unit = index // depth
        level = index % depth
        with jax.named_scope("project"):
            block = sbuf[unit].reshape(rows, width)
            start = pl.multiple_of(unit * rows, rows)
            k = jnp.dot(block, wk[level], preferred_element_type=F32)
            keys[level, pl.ds(start, rows), :] = k.astype(BF16)
            v = jnp.dot(block, wv[level], preferred_element_type=F32)
            values[level, :, pl.ds(start, rows)] = v.T.astype(BF16)

    def far_pair(j):
        return jnp.logical_and(edge, j == mirror)

    def query_copy(level, p, step):
        return remote(qbuf.at[level, p, s], qbuf.at[level, p, s], q_send.at[level, p, step],
                      q_recv.at[level, p, s], {"sp": lax.rem(s + step, sp)})

    def query_relay(level, p):
        return remote(qbuf.at[level, p, relay_to], qbuf.at[level, p, relay_to],
                      q_fsend.at[level, p], q_recv.at[level, p, relay_to], {"sp": relay_from})

    def each_query(level, p, act):
        for step in range(1, sp):
            copy = query_copy(level, p, step)
            if level == 0:
                act(copy)
            else:
                @pl.when(jnp.logical_not(far_pair(lax.rem(s + step, sp))))
                def _():
                    act(copy)

    def send_queries(level, p):
        each_query(level, p, lambda copy: copy.start())

    def drain_queries(level):
        for p in range(PIECES):
            each_query(level, p, lambda copy: copy.wait_send())
            if level > 0:
                @pl.when(relays)
                def _():
                    query_relay(level, p).wait_send()

    def result_copies(level, p, j):
        return (
            remote(osend.at[level, p, j], orecv.at[level, p, s], o_send.at[level, p, j],
                   o_recv.at[level, p, s], {"sp": j}),
            remote(ssend.at[level, p, j], srecv.at[level, p, s], e_send.at[level, p, j],
                   e_recv.at[level, p, s], {"sp": j}),
        )

    def relay_copies(level, p, j):
        return (
            remote(osend.at[level, p, j], orelay.at[level, p], o_send.at[level, p, j],
                   or_recv.at[level, p], {"sp": via}),
            remote(ssend.at[level, p, j], srelay.at[level, p], e_send.at[level, p, j],
                   er_recv.at[level, p], {"sp": via}),
        )

    def drain_results(level):
        for p in range(PIECES):
            for step in range(1, sp):
                for copy in result_copies(level, p, lax.rem(s + step, sp)):
                    copy.wait_send()

    def target_relay(step):
        slot = chip(step) * CORES + c
        return remote(tbuf.at[slot], tbuf.at[slot], t_fsend.at[step], t_recv.at[slot], partner)

    def source_relay(unit, piece):
        span = pl.ds(piece * (half // 2), half // 2)
        return remote(sbuf.at[unit, 0, span], sbuf.at[unit, 1, span], s_fsend.at[unit, piece],
                      s_recv.at[unit, 2 + piece], partner)

    def drain_relays():
        for step in range(1, nx):
            target_relay(step).wait_send()
        for unit in range(2, units):
            for piece in range(2):
                source_relay(unit, piece).wait_send()

    def first_queries():
        own_target.wait()
        for step in range(1, nx):
            slot = chip(step) * CORES + c
            arrived(tbuf.at[slot], t_recv.at[slot])
            target_relay(step).start()
        for step in range(nx):
            slot = chip(step) * CORES + partner_c
            arrived(tbuf.at[slot], t_recv.at[slot])

        @pl.loop(0, tp)
        def _(block):
            value = tbuf[block].astype(F32)
            ready = normalize(value, gains[0, 0:1, :]).astype(BF16)
            for p in range(PIECES):
                span = slice(p * prows, (p + 1) * prows)
                stream[p, block] = value[span]
                normed[p, block] = ready[span]

        load(0, 0).wait()
        q = jnp.dot(normed[...].reshape(PIECES * piece_rows, width), wq[0],
                    preferred_element_type=F32)
        for p in range(PIECES):
            qbuf[0, p, s] = q[p * piece_rows:(p + 1) * piece_rows].astype(BF16)
            send_queries(0, p)

        @pl.when(edge)
        def _():
            lowest = jnp.full((heads, 2 * piece_rows), LOWEST, F32)
            empty = jnp.concatenate([lowest, jnp.zeros_like(lowest)], axis=0)
            for level in range(depth):
                for p in range(PIECES):
                    orecv[level, p, mirror] = jnp.zeros((piece_rows, local_width), BF16)
                    srecv[level, p, mirror] = empty

    @pl.loop(0, units * depth - (depth - 1))
    def _(index):
        unit = index // depth
        level = index % depth

        @pl.when(index == 0)
        def _():
            for copy in own_source:
                copy.wait()
            load(1, 0).wait()
            load(2, 0).wait()
            load(0, 0).start()
            for later in range(1, depth):
                load(1, later).start()
                load(2, later).start()
            load(3, 0).start()
            for later in range(1, depth):
                load(0, later).start()
                load(3, later).start()

        for later in range(1, depth):
            @pl.when(index == later)
            def _():
                load(1, later).wait()
                load(2, later).wait()

        @pl.when(index == depth)
        def _():
            with jax.named_scope("first_queries"):
                first_queries()
            for part in range(2):
                arrived(sbuf.at[1, part], s_recv.at[1, part])

        @pl.when(jnp.logical_and(unit >= 2, level == 0))
        def _():
            with jax.named_scope("wait_remote"):
                for piece in range(2):
                    span = pl.ds(piece * (half // 2), half // 2)
                    arrived(sbuf.at[unit, 0, span], s_recv.at[unit, piece])
                    source_relay(unit, piece).start()
                for piece in range(2):
                    span = pl.ds(piece * (half // 2), half // 2)
                    arrived(sbuf.at[unit, 1, span], s_recv.at[unit, 2 + piece])

        project(index)

    drains += [drain_relays, functools.partial(drain_queries, 0)]

    def columns(parts):
        stacked = jnp.concatenate(parts, axis=0)
        fill = jnp.zeros((HEAD - stacked.shape[0], stacked.shape[1]), F32)
        return jnp.concatenate([stacked, fill], axis=0).T

    def weighted(cols, blocks, h):
        span = slice(h * HEAD, (h + 1) * HEAD)
        return sum(
            cols[0:piece_rows, k * heads + h:k * heads + h + 1] * block[:, span].astype(F32)
            for k, block in enumerate(blocks))

    def merge(layer, p):
        @pl.when(relays)
        def _():
          with jax.named_scope("merge"):
            arrived(orelay.at[layer, p], or_recv.at[layer, p])
            arrived(srelay.at[layer, p], er_recv.at[layer, p])
            mine, theirs = ssend[layer, p, relay_to], srelay[layer, p]
            top = jnp.maximum(mine[0:heads], theirs[0:heads])
            share = [jnp.exp2(one[0:heads] - top) for one in (mine, theirs)]
            total = share[0] * mine[heads:] + share[1] * theirs[heads:]
            cols = columns(share)
            blocks = (osend[layer, p, relay_to], orelay[layer, p])
            for h in range(heads):
                osend[layer, p, relay_to, :, h * HEAD:(h + 1) * HEAD] = weighted(
                    cols, blocks, h).astype(BF16)
            ssend[layer, p, relay_to] = jnp.concatenate([top, total], axis=0)
            for copy in result_copies(layer, p, relay_to):
                copy.start()

    def attend(layer, p, pair):
        first = 2 * pair
        for member in range(2):
            j = first + member

            @pl.when(j != s)
            def _():
                with jax.named_scope("wait_q"):
                    arrived(qbuf.at[layer, p, j], q_recv.at[layer, p, j])

            if layer > 0:
                @pl.when(jnp.logical_and(relays, j == relay_to))
                def _():
                    query_relay(layer, p).start()

        with jax.named_scope("attend"):
            q = qbuf[layer, p, pl.ds(first, 2)].reshape(2 * piece_rows, local_width)
            peaks, totals = [], []
            for h in range(heads):
                cols = slice(h * HEAD, (h + 1) * HEAD)
                scores = lax.dot_general(
                    keys[layer, :, cols], q[:, cols], (((1,), (1,)), ((), ())),
                    preferred_element_type=F32)
                peak = jnp.max(scores, axis=0, keepdims=True) * score_scale
                weights = jnp.exp2(scores * score_scale - peak)
                totals.append(jnp.sum(weights, axis=0, keepdims=True))
                peaks.append(peak)
                o = jnp.dot(values[layer, cols, :], weights.astype(BF16), preferred_element_type=F32)
                o = o.T.astype(BF16)
                for member in range(2):
                    osend[layer, p, first + member, :, cols] = o[member * piece_rows:(member + 1) * piece_rows]
            stats = jnp.concatenate(peaks + totals, axis=0)
            ssend[layer, p, first] = stats
            ssend[layer, p, first + 1] = pltpu.roll(stats, piece_rows, 1)

        for member in (1, 0):
            j = first + member

            @pl.when(j == s)
            def _():
                orecv[layer, p, s] = osend[layer, p, s]
                srecv[layer, p, s] = ssend[layer, p, s]

            @pl.when(far_pair(j))
            def _():
                for copy in relay_copies(layer, p, j):
                    copy.start()

            held = jnp.logical_or(far_pair(j), jnp.logical_and(relays, j == relay_to))

            @pl.when(jnp.logical_not(jnp.logical_or(held, j == s)))
            def _():
                for copy in result_copies(layer, p, j):
                    copy.start()

    def out_project(layer, p):
        with jax.named_scope("wait_o"):
            for step in range(1, sp):
                j = lax.rem(s + step, sp)

                @pl.when(jnp.logical_not(far_pair(j)))
                def _():
                    arrived(orecv.at[layer, p, j], o_recv.at[layer, p, j])
                    arrived(srecv.at[layer, p, j], e_recv.at[layer, p, j])
        with jax.named_scope("combine_out"):
            stats = [srecv[layer, p, j] for j in range(sp)]
            top = functools.reduce(jnp.maximum, [one[0:heads] for one in stats])
            share = [jnp.exp2(one[0:heads] - top) for one in stats]
            total = sum(part * one[heads:] for part, one in zip(share, stats))
            cols = columns([part / total for part in share])
            blocks = [orecv[layer, p, j] for j in range(sp)]
            for h in range(heads):
                attended[:, h * HEAD:(h + 1) * HEAD] = weighted(cols, blocks, h).astype(BF16)
            tile = min(512, width)
            for n in range(width // tile):
                span = slice(n * tile, (n + 1) * tile)
                part = jnp.dot(attended[...], wo[layer, :, span], preferred_element_type=F32).astype(BF16)
                for b in range(nx):
                    for core in range(CORES):
                        at = (b * CORES + core) * prows
                        pbuf[layer, p, core, b, :, span] = part[at:at + prows]
            go(remote(pbuf.at[layer, p, partner_c], half_in.at[layer, p], h_send.at[layer, p],
                      h_recv.at[layer, p], partner))

    def chip_total(layer, p):
        with jax.named_scope("chip_total"):
            arrived(half_in.at[layer, p], h_recv.at[layer, p])
            for b in range(nx):
                both_cores = pbuf[layer, p, c, b].astype(F32) + half_in[layer, p, b].astype(F32)
                chip_sum[layer, p, x, c, b] = both_cores.astype(BF16)
            own = chip_sum.at[layer, p, x, c]
            for step in range(1, nx):
                go(remote(own, own, c_send.at[layer, p, step], c_recv.at[layer, p, x], peer(step)))
            go(remote(own, own, c_psend.at[layer, p], c_frecv.at[layer, p, x], partner))

    def next_queries(layer, p):
        with jax.named_scope("xwait"):
            for step in range(1, nx):
                a = chip(step)
                other = chip_sum.at[layer, p, a, c]
                arrived(other, c_recv.at[layer, p, a])
                go(remote(other, other, c_fsend.at[layer, p, step], c_frecv.at[layer, p, a], partner))
            for step in range(nx):
                a = chip(step)
                arrived(chip_sum.at[layer, p, a, partner_c], c_frecv.at[layer, p, a])
        with jax.named_scope("norm_q"):
            for block in range(tp):
                projected = sum(
                    chip_sum[layer, p, a, block % CORES, block // CORES].astype(F32) for a in range(nx))
                value = stream[p, block] + normalize(projected, gains[layer, 1:2, :])
                stream[p, block] = value
                normed[p, block] = normalize(value, gains[layer + 1, 0:1, :]).astype(BF16)
            q = jnp.dot(normed[p].reshape(piece_rows, width), wq[layer + 1],
                        preferred_element_type=F32)
            qbuf[layer + 1, p, s] = q.astype(BF16)
            send_queries(layer + 1, p)

    def final_send(layer, p):
        with jax.named_scope("final_send"):
            arrived(half_in.at[layer, p], h_recv.at[layer, p])
            for step in range(1, nx):
                b = chip(step)
                both_cores = pbuf[layer, p, c, b].astype(F32) + half_in[layer, p, b].astype(F32)
                fin[0, p, b] = both_cores.astype(BF16)
                go(remote(fin.at[0, p, b], fin.at[1, p, x], f_send.at[p, step], f_recv.at[p, x],
                          peer(step)))

    def final_rows(layer, p):
        with jax.named_scope("final_rows"):
            projected = pbuf[layer, p, c, x].astype(F32) + half_in[layer, p, x].astype(F32)
            for step in range(1, nx):
                b = chip(step)
                arrived(fin.at[1, p, b], f_recv.at[p, b])
                projected = projected + fin[1, p, b].astype(F32)
            value = stream[p, t] + normalize(projected, gains[layer, 1:2, :])
            out[p * prows:(p + 1) * prows, :] = value.astype(out.dtype)

    for layer in range(depth):
        last = layer == depth - 1
        own_pair = s // 2

        @pl.loop(0, PIECES * pairs)
        def _(i):
            p = i // pairs
            k = i % pairs
            attend(layer, p, lax.rem(own_pair + k + (1 if layer == 0 else 0), pairs))
            for later in range(1, PIECES):
                @pl.when(i == later * pairs)
                def _():
                    merge(layer, later - 1)

        drains.append(functools.partial(drain_results, layer))
        if layer == 0:
            @pl.loop(units * depth - (depth - 1), units * depth)
            def _(index):
                project(index)
        merge(layer, PIECES - 1)
        load(3, layer).wait()

        for p in range(PIECES):
            out_project(layer, p)
            if last:
                final_send(layer, p)
            else:
                chip_total(layer, p)
        if not last:
            load(0, layer + 1).wait()
        for p in range(PIECES):
            if last:
                final_rows(layer, p)
            else:
                next_queries(layer, p)
        if not last:
            drains.append(functools.partial(drain_queries, layer + 1))

    finish()


def fused_body(nx, sp, target, source, w_query, w_key, w_value, w_out, gains):
    depth, width, local_width = w_query.shape
    trows, rows = target.shape[0], source.shape[0]
    tp = nx * CORES
    prows = trows // PIECES
    piece_rows = tp * prows
    heads = local_width // HEAD
    units = 2 * nx
    vmem = pltpu.VMEM
    dma = pltpu.SemaphoreType.DMA
    anywhere = pl.BlockSpec(memory_space=pl.ANY)
    whole = pl.BlockSpec(memory_space=pltpu.VMEM)
    results = (depth, PIECES, sp, piece_rows, local_width)
    notes = (depth, PIECES, sp, 2 * heads, 2 * piece_rows)
    return pl.pallas_call(
        functools.partial(fused_kernel, nx, sp, depth),
        out_shape=jax.ShapeDtypeStruct((trows, width), BF16),
        in_specs=[anywhere] * 6 + [whole],
        out_specs=whole,
        scratch_shapes=[
            vmem((tp, trows, width), BF16),
            vmem((units, 2, rows // 2, width), BF16),
            vmem(w_query.shape, BF16),
            vmem(w_key.shape, BF16),
            vmem(w_value.shape, BF16),
            vmem(w_out.shape, BF16),
            vmem((depth, units * rows, local_width), BF16),
            vmem((depth, local_width, units * rows), BF16),
            vmem((PIECES, tp, prows, width), F32),
            vmem((PIECES, tp, prows, width), BF16),
            vmem(results, BF16),
            vmem(results, BF16),
            vmem(results, BF16),
            vmem(notes, F32),
            vmem(notes, F32),
            vmem(results[:2] + results[3:], BF16),
            vmem(notes[:2] + notes[3:], F32),
            vmem((piece_rows, local_width), BF16),
            vmem((depth, PIECES, CORES, nx, prows, width), BF16),
            vmem((depth, PIECES, nx, prows, width), BF16),
            vmem((depth, PIECES, nx, CORES, nx, prows, width), BF16),
            vmem((2, PIECES, nx, prows, width), BF16),
            dma((3,)), dma((4, depth)),
            dma((nx,)), dma((tp,)), dma((nx,)),
            dma((2,)), dma((nx, 4)), dma((units, 4)), dma((units, 2)),
            dma((depth, PIECES, sp)), dma((depth, PIECES, sp)), dma((depth, PIECES)),
            dma((depth, PIECES, sp)), dma((depth, PIECES, sp)),
            dma((depth, PIECES, sp)), dma((depth, PIECES, sp)),
            dma((depth, PIECES)), dma((depth, PIECES)),
            dma((depth, PIECES)), dma((depth, PIECES)),
            dma((depth, PIECES, nx)), dma((depth, PIECES)), dma((depth, PIECES, nx)),
            dma((depth, PIECES, nx)), dma((depth, PIECES, nx)),
            dma((PIECES, nx)), dma((PIECES, nx)),
        ],
        compiler_params=pltpu.CompilerParams(
            collective_id=0, has_side_effects=True, vmem_limit_bytes=60 * 1024 * 1024),
    )(target, source, w_query, w_key, w_value, w_out, gains)


def split_heads(row_block):
    return row_block.reshape(row_block.shape[0], row_block.shape[1] // HEAD, HEAD)


def body(target, source, w_query, w_key, w_value, w_out, gains):
    local_width = w_query.shape[2]
    score_scale = HEAD ** (-0.5)
    depth = w_query.shape[0]
    project_shard_part = lax.all_gather(source, "tp", axis=0, tiled=True)
    layer_parts = [
        jnp.stack(
            [
                jnp.dot(project_shard_part, w_key[level], preferred_element_type=jnp.float32),
                jnp.dot(project_shard_part, w_value[level], preferred_element_type=jnp.float32),
            ]
        )
        for level in range(depth)
    ]
    projected_source = jnp.stack(layer_parts).astype(jnp.bfloat16)
    stream = target.astype(jnp.float32)
    for layer_index in range(depth):
        normed = normalize(stream, gains[layer_index, 0]).astype(jnp.bfloat16)
        query_weight = w_query[layer_index]
        queries = jnp.dot(
            lax.all_gather(normed, "tp", axis=0, tiled=True),
            query_weight,
            preferred_element_type=jnp.float32,
        ).astype(jnp.bfloat16)
        row_count = queries.shape[0]
        keys_here = projected_source[layer_index, 0]
        values_here = projected_source[layer_index, 1]
        every_query = lax.all_gather(queries, "sp", axis=0, tiled=True)
        scores = (
            jnp.einsum(
                "qhd,khd->hqk",
                split_heads(every_query),
                split_heads(keys_here),
                preferred_element_type=jnp.float32,
            )
            * score_scale
        )
        row_peak = lax.pmax(jnp.max(scores, axis=2), "sp")
        weights = jnp.exp(scores - row_peak[:, :, None])
        local_summed = jnp.einsum(
            "hqk,khd->hqd",
            weights.astype(jnp.bfloat16),
            split_heads(values_here),
            preferred_element_type=jnp.float32,
        )
        summed, row_total = (
            lax.psum_scatter(
                local_summed.astype(jnp.bfloat16), "sp", scatter_dimension=1, tiled=True
            ).astype(jnp.float32),
            lax.psum_scatter(
                jnp.sum(weights, axis=2).astype(jnp.bfloat16), "sp", scatter_dimension=1, tiled=True
            ).astype(jnp.float32),
        )
        heads_out = summed / row_total[:, :, None]
        attended = (
            jnp.transpose(heads_out, (1, 0, 2)).reshape(row_count, local_width).astype(jnp.bfloat16)
        )
        out_weight = w_out[layer_index]
        projected = lax.psum_scatter(
            jnp.dot(attended, out_weight, preferred_element_type=jnp.float32).astype(jnp.bfloat16),
            "tp",
            scatter_dimension=0,
            tiled=True,
        ).astype(jnp.float32)
        stream = stream + normalize(projected, gains[layer_index, 1])
    return stream.astype(jnp.bfloat16)


def solution(mesh):
    in_specs = (
        P(("grp", "sp", "tp"), None),
        P(("grp", "sp", "tp"), None),
        P(None, None, "tp"),
        P(None, None, "tp"),
        P(None, None, "tp"),
        P(None, "tp", None),
        P(),
    )
    out_specs = P(("grp", "sp", "tp"), None)
    sp, tp = mesh.shape["sp"], mesh.shape["tp"]

    def run(target, source, w_query, w_key, w_value, w_out, gains):
        trows, rows, local_width = target.shape[0], source.shape[0], w_query.shape[2]
        tiles = (trows % (16 * PIECES) == 0 and tp * trows == PIECES * (HEAD // 2) and rows % 128 == 0
                 and sp % 2 == 0 and sp >= 4
                 and local_width % (4 * HEAD) == 0 and tp % CORES == 0)
        form = functools.partial(fused_body, tp // CORES, sp) if tiles else body
        return form(target, source, w_query, w_key, w_value, w_out, gains)

    return jax.shard_map(run, mesh=mesh, in_specs=in_specs, out_specs=out_specs, check_vma=False)
```

```python
import functools
import math

import jax
import jax.numpy as jnp
from jax import lax
from jax.experimental import pallas as pl
from jax.experimental.pallas import tpu as pltpu
from jax.sharding import PartitionSpec as P

HEAD = 128
CORES = 2
PIECES = 2
MERGED = (2, 2)


EPS = 1e-06
MESH = pl.DeviceIdType.MESH
F32 = jnp.float32
LOWEST = -1e30
BF16 = jnp.bfloat16


def normalize(row_block, gain_row):
    return (
        row_block
        * lax.rsqrt(jnp.mean(row_block * row_block, axis=-1, keepdims=True) + EPS)
        * gain_row
    )


def fused_kernel(
    nx, sp, depth,
    target, source, w_query, w_key, w_value, w_out, gains, out,
    tbuf, sbuf, wq, wk, wv, wo, keys, values, stream, normed, qbuf,
    osend, orecv, ssend, srecv, orelay, srelay, attended, pbuf, half_in, chip_sum, fin, ledger,
    local_sem, weight_sem, send_sem, t_recv, s_recv, p_recv, r_recv, first_recv, q_recv,
    o_recv, m_recv, h_recv, c_recv, d_recv, f_recv,
):
    s = lax.axis_index("sp")
    t = lax.axis_index("tp")
    x = t // CORES
    c = t % CORES
    partner_c = 1 - c
    partner = {"tp": x * CORES + partner_c}
    units = sbuf.shape[0]
    half = sbuf.shape[2]
    width = sbuf.shape[3]
    rows = 2 * half
    local_width = wk.shape[2]
    heads = local_width // HEAD
    tp = nx * CORES
    prows = stream.shape[2]
    piece_rows = tp * prows
    score_scale = HEAD ** (-0.5) * math.log2(math.e)

    pairs = sp // 2
    edge = jnp.logical_or(s == 0, s == sp - 1)
    mirror = sp - 1 - s
    relays = jnp.logical_or(s == 1, s == sp - 2)
    relay_from = jnp.where(s == 1, 0, sp - 1)
    relay_to = sp - 1 - relay_from
    via = jnp.where(s == 0, 1, sp - 2)

    def chip(step):
        return lax.rem(x + step, nx)

    def peer(step):
        return {"tp": chip(step) * CORES + c}

    def remote(src, dst, send_sem, recv_sem, device):
        return pltpu.make_async_remote_copy(
            src_ref=src, dst_ref=dst, send_sem=send_sem, recv_sem=recv_sem,
            device_id=device, device_id_type=MESH,
        )

    def arrived(sem, *shapes):
        total = sum(math.prod(shape) * size for shape, size in shapes)
        block = ledger.at[pl.ds(0, total // math.prod(ledger.shape[1:]) // 4)]
        pltpu.make_async_copy(block, block, sem).wait()

    target_rows = (tbuf.shape[1:], 2)
    source_part = (sbuf.shape[2:], 2)
    result_block = (osend.shape[3:], 2)
    stats_block = (ssend.shape[3:], 4)
    sum_block = (half_in.shape[3:], 2)
    chip_rows = (half_in.shape[2:], 2)
    weight_block = (wk.shape[1:], 2)

    own_target = pltpu.make_async_copy(target, tbuf.at[t], local_sem.at[0])
    own_source = [
        pltpu.make_async_copy(
            source.at[pl.ds(part * half, half)], sbuf.at[0, part], local_sem.at[1])
        for part in range(2)
    ]

    def load(kind, level):
        pair = ((w_query, wq), (w_key, wk), (w_value, wv), (w_out, wo))[kind]
        return pltpu.make_async_copy(
            pair[0].at[level], pair[1].at[level], weight_sem.at[(0, 1, 1, 2)[kind], level])

    own_target.start()
    for copy in own_source:
        copy.start()
    load(1, 0).start()
    load(2, 0).start()

    barrier = pltpu.get_barrier_semaphore()
    pl.semaphore_signal(barrier, inc=1, device_id=partner, device_id_type=MESH)
    for step in range(1, nx):
        pl.semaphore_signal(barrier, inc=1, device_id=peer(step), device_id_type=MESH)
    for step in range(1, sp):
        pl.semaphore_signal(
            barrier, inc=1, device_id={"sp": lax.rem(s + step, sp)}, device_id_type=MESH)
    with jax.named_scope("barrier"):
        pl.semaphore_wait(barrier, 1 + (nx - 1) + (sp - 1))

    SOURCE, LINE, ROW = range(3)
    sent = {SOURCE: [], LINE: [], ROW: []}

    def go(copy, kind, shape):
        copy.start()
        sent[kind].append(shape)

    for step in range(1, nx):
        go(remote(target, tbuf.at[t], send_sem.at[SOURCE], t_recv.at[step], peer(step)),
           SOURCE, target_rows)
    go(remote(target, tbuf.at[t], send_sem.at[SOURCE], t_recv.at[0], partner), SOURCE, target_rows)
    for part in range(2):
        block = source.at[pl.ds(part * half, half)]
        for piece in range(2):
            span = pl.ds(piece * (half // 2), half // 2)
            for step in range(1, nx):
                unit = 2 * (nx - step) + part
                go(remote(block.at[span], sbuf.at[unit, 0, span], send_sem.at[SOURCE],
                          s_recv.at[unit - 2, piece], peer(step)),
                   SOURCE, ((half // 2, width), 2))
        go(remote(block, sbuf.at[1, part], send_sem.at[SOURCE], p_recv.at[0], partner),
           SOURCE, source_part)

    def project(index):
        unit = index // depth
        level = index % depth
        with jax.named_scope("project"):
            block = sbuf[unit].reshape(rows, width)
            start = pl.multiple_of(unit * rows, rows)
            k = jnp.dot(block, wk[level], preferred_element_type=F32)
            keys[level, pl.ds(start, rows), :] = k.astype(BF16)
            v = jnp.dot(block, wv[level], preferred_element_type=F32)
            values[level, :, pl.ds(start, rows)] = v.T.astype(BF16)

    def far_pair(j):
        return jnp.logical_and(edge, j == mirror)

    def query_copy(level, p, j):
        sem = first_recv.at[0] if level == 0 else q_recv.at[level - 1, p, s]
        return remote(qbuf.at[level, p, s], qbuf.at[level, p, s], send_sem.at[LINE], sem, {"sp": j})

    def forward(level, p):
        @pl.when(relays)
        def _():
            arrived(q_recv.at[level - 1, p, relay_to], result_block)
            block = qbuf.at[level, p, relay_to]
            remote(block, block, send_sem.at[LINE], q_recv.at[level - 1, p, relay_to],
                   {"sp": relay_from}).start()

    def send_queries(level, p):
        for distance in range(sp - 1 if level == 0 else sp - 2, 0, -1):
            @pl.when(s + distance < sp)
            def _():
                query_copy(level, p, lax.rem(s + distance, sp)).start()

            @pl.when(s >= distance)
            def _():
                query_copy(level, p, lax.rem(s + sp - distance, sp)).start()

    def drain_line():
        def drain(queries):
            blocks = PIECES * ((depth + 1) * (sp - 1) + (depth - 1) * queries)
            arrived(send_sem.at[LINE], *([result_block] * blocks),
                    *([stats_block] * (depth * PIECES * (sp - 1))))

        @pl.when(edge)
        def _():
            drain(sp - 2)

        @pl.when(relays)
        def _():
            drain(sp)

        if sp > 4:
            @pl.when(jnp.logical_not(jnp.logical_or(edge, relays)))
            def _():
                drain(sp - 1)

    def merged(level, p):
        return p < MERGED[min(level, 1)]

    def result_copies(level, p, j):
        return (
            remote(osend.at[level, p, j], orecv.at[level, p, s], send_sem.at[LINE],
                   o_recv.at[level, p], {"sp": j}),
            remote(ssend.at[level, p, j], srecv.at[level, p, s], send_sem.at[LINE],
                   o_recv.at[level, p], {"sp": j}),
        )

    def relay_copies(level, p, j):
        return (
            remote(osend.at[level, p, j], orelay.at[level, p], send_sem.at[LINE],
                   m_recv.at[level, p], {"sp": via}),
            remote(ssend.at[level, p, j], srelay.at[level, p], send_sem.at[LINE],
                   m_recv.at[level, p], {"sp": via}),
        )

    def source_relay(unit, piece):
        span = pl.ds(piece * (half // 2), half // 2)
        return remote(sbuf.at[unit, 0, span], sbuf.at[unit, 1, span], send_sem.at[SOURCE],
                      r_recv.at[unit - 2], partner)

    def first_queries():
        own_target.wait()
        for step in range(1, nx):
            slot = chip(step) * CORES + c
            arrived(t_recv.at[step], target_rows)
            go(remote(tbuf.at[slot], tbuf.at[slot], send_sem.at[SOURCE], t_recv.at[0], partner),
               SOURCE, target_rows)
        arrived(t_recv.at[0], *([target_rows] * nx))

        @pl.loop(0, tp)
        def _(block):
            value = tbuf[block].astype(F32)
            ready = normalize(value, gains[0, 0:1, :]).astype(BF16)
            for p in range(PIECES):
                span = slice(p * prows, (p + 1) * prows)
                stream[p, block] = value[span]
                normed[p, block] = ready[span]

        load(0, 0).wait()
        q = jnp.dot(normed[...].reshape(PIECES * piece_rows, width), wq[0],
                    preferred_element_type=F32)
        for p in range(PIECES):
            qbuf[0, p, s] = q[p * piece_rows:(p + 1) * piece_rows].astype(BF16)
            send_queries(0, p)

        @pl.when(edge)
        def _():
            lowest = jnp.full((heads, 2 * piece_rows), LOWEST, F32)
            empty = jnp.concatenate([lowest, jnp.zeros_like(lowest)], axis=0)
            for level in range(depth):
                for p in range(PIECES):
                    if merged(level, p):
                        orecv[level, p, mirror] = jnp.zeros((piece_rows, local_width), BF16)
                        srecv[level, p, mirror] = empty

    @pl.loop(0, units * depth - (depth - 1))
    def _(index):
        unit = index // depth
        level = index % depth

        @pl.when(index == 0)
        def _():
            arrived(local_sem.at[1], source_part, source_part)
            arrived(weight_sem.at[1, 0], weight_block, weight_block)
            load(0, 0).start()
            for later in range(1, depth):
                load(1, later).start()
                load(2, later).start()
            load(3, 0).start()
            for later in range(1, depth):
                load(0, later).start()
                load(3, later).start()

        for later in range(1, depth):
            @pl.when(index == later)
            def _():
                arrived(weight_sem.at[1, later], weight_block, weight_block)

        @pl.when(index == depth)
        def _():
            with jax.named_scope("first_queries"):
                first_queries()
            arrived(p_recv.at[0], source_part, source_part)

        @pl.when(jnp.logical_and(unit >= 2, level == 0))
        def _():
            with jax.named_scope("wait_remote"):
                for piece in range(2):
                    arrived(s_recv.at[unit - 2, piece], ((half // 2, width), 2))
                    source_relay(unit, piece).start()
                arrived(r_recv.at[unit - 2], source_part)

        project(index)

    sent[SOURCE] += [source_part] * (units - 2)
    arrived(first_recv.at[0], *([result_block] * (PIECES * (sp - 1))))

    def columns(parts):
        stacked = jnp.concatenate(parts, axis=0)
        fill = jnp.zeros((HEAD - stacked.shape[0], stacked.shape[1]), F32)
        return jnp.concatenate([stacked, fill], axis=0).T

    def weighted(cols, blocks, h):
        span = slice(h * HEAD, (h + 1) * HEAD)
        return sum(
            cols[0:piece_rows, k * heads + h:k * heads + h + 1] * block[:, span].astype(F32)
            for k, block in enumerate(blocks))

    def merge(layer, p):
        @pl.when(relays)
        def _():
          with jax.named_scope("merge"):
            arrived(m_recv.at[layer, p], result_block, stats_block)
            mine, theirs = ssend[layer, p, relay_to], srelay[layer, p]
            top = jnp.maximum(mine[0:heads], theirs[0:heads])
            share = [jnp.exp2(one[0:heads] - top) for one in (mine, theirs)]
            total = share[0] * mine[heads:] + share[1] * theirs[heads:]
            cols = columns(share)
            blocks = (osend[layer, p, relay_to], orelay[layer, p])
            for h in range(heads):
                osend[layer, p, relay_to, :, h * HEAD:(h + 1) * HEAD] = weighted(
                    cols, blocks, h).astype(BF16)
            ssend[layer, p, relay_to] = jnp.concatenate([top, total], axis=0)
            for copy in result_copies(layer, p, relay_to):
                copy.start()

    def attend(layer, p, pair):
        first = 2 * pair
        for member in range(2):
            j = first + member
            if layer > 0:
                taken = jnp.logical_or(j == s, jnp.logical_and(relays, j == relay_to))

                @pl.when(jnp.logical_not(taken))
                def _():
                    with jax.named_scope("wait_q"):
                        arrived(q_recv.at[layer - 1, p, j], result_block)

        with jax.named_scope("attend"):
            q = qbuf[layer, p, pl.ds(first, 2)].reshape(2 * piece_rows, local_width)
            peaks, totals = [], []
            for h in range(heads):
                cols = slice(h * HEAD, (h + 1) * HEAD)
                scores = lax.dot_general(
                    keys[layer, :, cols], q[:, cols], (((1,), (1,)), ((), ())),
                    preferred_element_type=F32)
                peak = jnp.max(scores, axis=0, keepdims=True) * score_scale
                weights = jnp.exp2(scores * score_scale - peak)
                totals.append(jnp.sum(weights, axis=0, keepdims=True))
                peaks.append(peak)
                o = jnp.dot(values[layer, cols, :], weights.astype(BF16), preferred_element_type=F32)
                o = o.T.astype(BF16)
                for member in range(2):
                    osend[layer, p, first + member, :, cols] = o[member * piece_rows:(member + 1) * piece_rows]
            stats = jnp.concatenate(peaks + totals, axis=0)
            ssend[layer, p, first] = stats
            ssend[layer, p, first + 1] = pltpu.roll(stats, piece_rows, 1)

        for member in (1, 0):
            j = first + member

            @pl.when(j == s)
            def _():
                orecv[layer, p, s] = osend[layer, p, s]
                srecv[layer, p, s] = ssend[layer, p, s]

            aside = jnp.logical_and(far_pair(j), merged(layer, p))
            held = jnp.logical_and(jnp.logical_and(relays, j == relay_to), merged(layer, p))

            @pl.when(aside)
            def _():
                for copy in relay_copies(layer, p, j):
                    copy.start()

            @pl.when(jnp.logical_not(functools.reduce(jnp.logical_or, (j == s, aside, held))))
            def _():
                for copy in result_copies(layer, p, j):
                    copy.start()

    def out_project(layer, p):
        with jax.named_scope("wait_o"):
            if merged(layer, p):
                @pl.when(edge)
                def _():
                    arrived(o_recv.at[layer, p], *([result_block, stats_block] * (sp - 2)))

                @pl.when(jnp.logical_not(edge))
                def _():
                    arrived(o_recv.at[layer, p], *([result_block, stats_block] * (sp - 1)))
            else:
                arrived(o_recv.at[layer, p], *([result_block, stats_block] * (sp - 1)))
        with jax.named_scope("combine_out"):
            stats = [srecv[layer, p, j] for j in range(sp)]
            top = functools.reduce(jnp.maximum, [one[0:heads] for one in stats])
            share = [jnp.exp2(one[0:heads] - top) for one in stats]
            total = sum(part * one[heads:] for part, one in zip(share, stats))
            cols = columns([part / total for part in share])
            blocks = [orecv[layer, p, j] for j in range(sp)]
            for h in range(heads):
                attended[:, h * HEAD:(h + 1) * HEAD] = weighted(cols, blocks, h).astype(BF16)
            tile = min(512, width)
            for n in range(width // tile):
                span = slice(n * tile, (n + 1) * tile)
                part = jnp.dot(attended[...], wo[layer, :, span], preferred_element_type=F32).astype(BF16)
                for b in range(nx):
                    for core in range(CORES):
                        at = (b * CORES + core) * prows
                        pbuf[layer, p, core, b, :, span] = part[at:at + prows]
            go(remote(pbuf.at[layer, p, partner_c], half_in.at[layer, p], send_sem.at[ROW],
                      h_recv.at[layer, p], partner), ROW, chip_rows)

    def chip_total(layer, p):
        with jax.named_scope("chip_total"):
            arrived(h_recv.at[layer, p], chip_rows)
            for b in range(nx):
                both_cores = pbuf[layer, p, c, b].astype(F32) + half_in[layer, p, b].astype(F32)
                chip_sum[layer, p, x, c, b] = both_cores.astype(BF16)
            own = chip_sum.at[layer, p, x, c]
            for step in range(1, nx):
                go(remote(own, own, send_sem.at[ROW], c_recv.at[layer, p, nx - step - 1], peer(step)),
                   ROW, chip_rows)
            go(remote(own, own, send_sem.at[ROW], d_recv.at[layer, p], partner), ROW, chip_rows)

    def next_queries(layer, p):
        with jax.named_scope("xwait"):
            for step in range(1, nx):
                a = chip(step)
                other = chip_sum.at[layer, p, a, c]
                arrived(c_recv.at[layer, p, step - 1], chip_rows)
                go(remote(other, other, send_sem.at[ROW], d_recv.at[layer, p], partner), ROW, chip_rows)
            arrived(d_recv.at[layer, p], *([chip_rows] * nx))
        with jax.named_scope("norm_q"):
            for block in range(tp):
                projected = sum(
                    chip_sum[layer, p, a, block % CORES, block // CORES].astype(F32) for a in range(nx))
                value = stream[p, block] + normalize(projected, gains[layer, 1:2, :])
                stream[p, block] = value
                normed[p, block] = normalize(value, gains[layer + 1, 0:1, :]).astype(BF16)
            q = jnp.dot(normed[p].reshape(piece_rows, width), wq[layer + 1],
                        preferred_element_type=F32)
            qbuf[layer + 1, p, s] = q.astype(BF16)
            send_queries(layer + 1, p)

    def final_send(layer, p):
        with jax.named_scope("final_send"):
            arrived(h_recv.at[layer, p], chip_rows)
            for step in range(1, nx):
                b = chip(step)
                both_cores = pbuf[layer, p, c, b].astype(F32) + half_in[layer, p, b].astype(F32)
                fin[0, p, b] = both_cores.astype(BF16)
                go(remote(fin.at[0, p, b], fin.at[1, p, x], send_sem.at[ROW],
                          f_recv.at[p, nx - step - 1], peer(step)), ROW, sum_block)

    def final_rows(layer, p):
        with jax.named_scope("final_rows"):
            projected = pbuf[layer, p, c, x].astype(F32) + half_in[layer, p, x].astype(F32)
            for step in range(1, nx):
                b = chip(step)
                arrived(f_recv.at[p, step - 1], sum_block)
                projected = projected + fin[1, p, b].astype(F32)
            value = stream[p, t] + normalize(projected, gains[layer, 1:2, :])
            out[p * prows:(p + 1) * prows, :] = value.astype(out.dtype)

    for layer in range(depth):
        last = layer == depth - 1
        own_pair = s // 2
        count = PIECES * pairs

        @pl.loop(0, count)
        def _(i):
            if layer == 0:
                p, k = i // pairs, i % pairs + 1
            else:
                p, k = i % PIECES, i // PIECES
                for later in range(PIECES):
                    @pl.when(i == (0 if later == 0 else count - PIECES + later))
                    def _():
                        forward(layer, later)
            attend(layer, p, lax.rem(own_pair + k, pairs))
            if layer == 0:
                for later in range(1, PIECES):
                    if merged(layer, later - 1):
                        @pl.when(i == later * pairs)
                        def _():
                            merge(layer, later - 1)

        if layer == 0:
            @pl.loop(units * depth - (depth - 1), units * depth)
            def _(index):
                project(index)
        for p in range(PIECES):
            if merged(layer, p) and (layer > 0 or p == PIECES - 1):
                merge(layer, p)
        load(3, layer).wait()

        for p in range(PIECES):
            out_project(layer, p)
            if last:
                final_send(layer, p)
            else:
                chip_total(layer, p)
        if not last:
            load(0, layer + 1).wait()
        for p in range(PIECES):
            if last:
                final_rows(layer, p)
            else:
                next_queries(layer, p)

    with jax.named_scope("finish"):
        drain_line()
        for kind in (SOURCE, ROW):
            arrived(send_sem.at[kind], *sent[kind])


def fused_body(nx, sp, target, source, w_query, w_key, w_value, w_out, gains):
    depth, width, local_width = w_query.shape
    trows, rows = target.shape[0], source.shape[0]
    tp = nx * CORES
    prows = trows // PIECES
    piece_rows = tp * prows
    heads = local_width // HEAD
    units = 2 * nx
    vmem = pltpu.VMEM
    dma = pltpu.SemaphoreType.DMA
    anywhere = pl.BlockSpec(memory_space=pl.ANY)
    whole = pl.BlockSpec(memory_space=pltpu.VMEM)
    results = (depth, PIECES, sp, piece_rows, local_width)
    notes = (depth, PIECES, sp, 2 * heads, 2 * piece_rows)
    return pl.pallas_call(
        functools.partial(fused_kernel, nx, sp, depth),
        out_shape=jax.ShapeDtypeStruct((trows, width), BF16),
        in_specs=[anywhere] * 6 + [whole],
        out_specs=whole,
        scratch_shapes=[
            vmem((tp, trows, width), BF16),
            vmem((units, 2, rows // 2, width), BF16),
            vmem(w_query.shape, BF16),
            vmem(w_key.shape, BF16),
            vmem(w_value.shape, BF16),
            vmem(w_out.shape, BF16),
            vmem((depth, units * rows, local_width), BF16),
            vmem((depth, local_width, units * rows), BF16),
            vmem((PIECES, tp, prows, width), F32),
            vmem((PIECES, tp, prows, width), BF16),
            vmem(results, BF16),
            vmem(results, BF16),
            vmem(results, BF16),
            vmem(notes, F32),
            vmem(notes, F32),
            vmem(results[:2] + results[3:], BF16),
            vmem(notes[:2] + notes[3:], F32),
            vmem((piece_rows, local_width), BF16),
            vmem((depth, PIECES, CORES, nx, prows, width), BF16),
            vmem((depth, PIECES, nx, prows, width), BF16),
            vmem((depth, PIECES, nx, CORES, nx, prows, width), BF16),
            vmem((2, PIECES, nx, prows, width), BF16),
            vmem((1024, 8, 128), F32),
            dma((2,)), dma((3, depth)), dma((3,)), dma((nx,)),
            dma((units - 2, 2)), dma((1,)), dma((units - 2,)), dma((1,)), dma((depth - 1, PIECES, sp)),
            dma((depth, PIECES)), dma((depth, PIECES)), dma((depth, PIECES)),
            dma((depth - 1, PIECES, nx - 1)), dma((depth - 1, PIECES)), dma((PIECES, nx - 1)),
        ],
        compiler_params=pltpu.CompilerParams(
            collective_id=0, has_side_effects=True, vmem_limit_bytes=60 * 1024 * 1024),
    )(target, source, w_query, w_key, w_value, w_out, gains)


def split_heads(row_block):
    return row_block.reshape(row_block.shape[0], row_block.shape[1] // HEAD, HEAD)


def body(target, source, w_query, w_key, w_value, w_out, gains):
    local_width = w_query.shape[2]
    score_scale = HEAD ** (-0.5)
    depth = w_query.shape[0]
    project_shard_part = lax.all_gather(source, "tp", axis=0, tiled=True)
    layer_parts = [
        jnp.stack(
            [
                jnp.dot(project_shard_part, w_key[level], preferred_element_type=jnp.float32),
                jnp.dot(project_shard_part, w_value[level], preferred_element_type=jnp.float32),
            ]
        )
        for level in range(depth)
    ]
    projected_source = jnp.stack(layer_parts).astype(jnp.bfloat16)
    stream = target.astype(jnp.float32)
    for layer_index in range(depth):
        normed = normalize(stream, gains[layer_index, 0]).astype(jnp.bfloat16)
        query_weight = w_query[layer_index]
        queries = jnp.dot(
            lax.all_gather(normed, "tp", axis=0, tiled=True),
            query_weight,
            preferred_element_type=jnp.float32,
        ).astype(jnp.bfloat16)
        row_count = queries.shape[0]
        keys_here = projected_source[layer_index, 0]
        values_here = projected_source[layer_index, 1]
        every_query = lax.all_gather(queries, "sp", axis=0, tiled=True)
        scores = (
            jnp.einsum(
                "qhd,khd->hqk",
                split_heads(every_query),
                split_heads(keys_here),
                preferred_element_type=jnp.float32,
            )
            * score_scale
        )
        row_peak = lax.pmax(jnp.max(scores, axis=2), "sp")
        weights = jnp.exp(scores - row_peak[:, :, None])
        local_summed = jnp.einsum(
            "hqk,khd->hqd",
            weights.astype(jnp.bfloat16),
            split_heads(values_here),
            preferred_element_type=jnp.float32,
        )
        summed, row_total = (
            lax.psum_scatter(
                local_summed.astype(jnp.bfloat16), "sp", scatter_dimension=1, tiled=True
            ).astype(jnp.float32),
            lax.psum_scatter(
                jnp.sum(weights, axis=2).astype(jnp.bfloat16), "sp", scatter_dimension=1, tiled=True
            ).astype(jnp.float32),
        )
        heads_out = summed / row_total[:, :, None]
        attended = (
            jnp.transpose(heads_out, (1, 0, 2)).reshape(row_count, local_width).astype(jnp.bfloat16)
        )
        out_weight = w_out[layer_index]
        projected = lax.psum_scatter(
            jnp.dot(attended, out_weight, preferred_element_type=jnp.float32).astype(jnp.bfloat16),
            "tp",
            scatter_dimension=0,
            tiled=True,
        ).astype(jnp.float32)
        stream = stream + normalize(projected, gains[layer_index, 1])
    return stream.astype(jnp.bfloat16)


def solution(mesh):
    in_specs = (
        P(("grp", "sp", "tp"), None),
        P(("grp", "sp", "tp"), None),
        P(None, None, "tp"),
        P(None, None, "tp"),
        P(None, None, "tp"),
        P(None, "tp", None),
        P(),
    )
    out_specs = P(("grp", "sp", "tp"), None)
    sp, tp = mesh.shape["sp"], mesh.shape["tp"]

    def run(target, source, w_query, w_key, w_value, w_out, gains):
        trows, rows, local_width = target.shape[0], source.shape[0], w_query.shape[2]
        tiles = (trows % (16 * PIECES) == 0 and tp * trows == PIECES * (HEAD // 2) and rows % 128 == 0
                 and sp % 2 == 0 and sp >= 4 and w_query.shape[0] > 1 and tp > CORES
                 and local_width % (4 * HEAD) == 0 and tp % CORES == 0)
        form = functools.partial(fused_body, tp // CORES, sp) if tiles else body
        return form(target, source, w_query, w_key, w_value, w_out, gains)

    return jax.shard_map(run, mesh=mesh, in_specs=in_specs, out_specs=out_specs, check_vma=False)
```

```python
import functools
import math

import jax
import jax.numpy as jnp
from jax import lax
from jax.experimental import pallas as pl
from jax.experimental.pallas import tpu as pltpu
from jax.sharding import PartitionSpec as P

HEAD = 128
CORES = 2
PIECES = 2
VMEM_KIB = 54100


EPS = 1e-06
MESH = pl.DeviceIdType.MESH
F32 = jnp.float32
BF16 = jnp.bfloat16


def normalize(row_block, gain_row):
    return (
        row_block
        * lax.rsqrt(jnp.mean(row_block * row_block, axis=-1, keepdims=True) + EPS)
        * gain_row
    )


def fused_kernel(
    nx, sp, depth,
    target, source, w_query, w_key, w_value, w_out, gain_rows, out,
    tbuf, sbuf, wq, wk, wv, wo, keys, values, stream, normed, qbuf,
    osend, orecv, ssend, srecv, orelay, srelay, attended, pbuf, half_in, chip_sum, fin, ledger, gains,
    local_sem, weight_sem, send_sem, t_recv, s_recv, p_recv, r_recv, first_recv, q_recv,
    o_recv, m_recv, h_recv, c_recv, d_recv, f_recv,
):
    s = lax.axis_index("sp")
    t = lax.axis_index("tp")
    x = t // CORES
    c = t % CORES
    partner_c = 1 - c
    partner = {"tp": x * CORES + partner_c}
    units = sbuf.shape[0]
    half = sbuf.shape[2]
    width = sbuf.shape[3]
    rows = 2 * half
    local_width = wk.shape[2]
    heads = local_width // HEAD
    tp = nx * CORES
    prows = stream.shape[2]
    piece_rows = tp * prows
    score_scale = HEAD ** (-0.5) * math.log2(math.e)

    pairs = sp // 2
    edge = jnp.logical_or(s == 0, s == sp - 1)
    inner = jnp.logical_not(edge)
    low = s < pairs
    near = jnp.where(s % 2 == 0, s + 1, s - 1)
    far_edge = jnp.where(low, sp - 1, 0)
    far_inner = jnp.where(low, pairs, pairs - 1)

    def chip(step):
        return lax.rem(x + step, nx)

    def peer(step):
        return {"tp": chip(step) * CORES + c}

    def remote(src, dst, send_sem, recv_sem, device):
        return pltpu.make_async_remote_copy(
            src_ref=src, dst_ref=dst, send_sem=send_sem, recv_sem=recv_sem,
            device_id=device, device_id_type=MESH,
        )

    def arrived(sem, *shapes):
        total = sum(math.prod(shape) * size for shape, size in shapes)
        block = ledger.at[pl.ds(0, total // math.prod(ledger.shape[1:]) // 4)]
        pltpu.make_async_copy(block, block, sem).wait()

    target_rows = (tbuf.shape[1:], 2)
    source_part = (sbuf.shape[2:], 2)
    result_block = (osend.shape[3:], 2)
    stats_block = (ssend.shape[3:], 4)
    sum_block = (half_in.shape[3:], 2)
    chip_rows = (half_in.shape[2:], 2)
    weight_block = (wk.shape[1:], 2)

    own_target = pltpu.make_async_copy(target, tbuf.at[t], local_sem.at[0])
    own_source = [
        pltpu.make_async_copy(
            source.at[pl.ds(part * half, half)], sbuf.at[0, part], local_sem.at[1])
        for part in range(2)
    ]

    def load(kind, level):
        pair = ((w_query, wq), (w_key, wk), (w_value, wv), (w_out, wo))[kind]
        return pltpu.make_async_copy(
            pair[0].at[level], pair[1].at[level], weight_sem.at[(0, 1, 1, 2)[kind], level])

    own_gains = pltpu.make_async_copy(gain_rows, gains, local_sem.at[2])
    own_target.start()
    own_gains.start()
    for copy in own_source:
        copy.start()
    load(1, 0).start()
    load(2, 0).start()

    barrier = pltpu.get_barrier_semaphore()
    pl.semaphore_signal(barrier, inc=1, device_id=partner, device_id_type=MESH)
    for step in range(1, nx):
        pl.semaphore_signal(barrier, inc=1, device_id=peer(step), device_id_type=MESH)
    for step in range(1, sp):
        pl.semaphore_signal(
            barrier, inc=1, device_id={"sp": lax.rem(s + step, sp)}, device_id_type=MESH)
    with jax.named_scope("barrier"):
        pl.semaphore_wait(barrier, 1 + (nx - 1) + (sp - 1))

    spans = ((0, half // 2), (half // 2, half // 4), (3 * half // 4, half // 8), (7 * half // 8, half // 8))
    SOURCE, LINE, ROW = range(3)
    sent = {SOURCE: [], LINE: [], ROW: []}

    def go(copy, kind, shape):
        copy.start()
        sent[kind].append(shape)

    for step in range(1, nx):
        go(remote(target, tbuf.at[t], send_sem.at[SOURCE], t_recv.at[step], peer(step)),
           SOURCE, target_rows)
    go(remote(target, tbuf.at[t], send_sem.at[SOURCE], t_recv.at[0], partner), SOURCE, target_rows)
    for part in range(2):
        block = source.at[pl.ds(part * half, half)]
        for piece, (at, size) in enumerate(spans):
            span = pl.ds(at, size)
            for step in range(1, nx):
                unit = 2 * (nx - step) + part
                go(remote(block.at[span], sbuf.at[unit, 0, span], send_sem.at[SOURCE],
                          s_recv.at[unit - 2, piece], peer(step)),
                   SOURCE, ((size, width), 2))
        go(remote(block, sbuf.at[1, part], send_sem.at[SOURCE], p_recv.at[0], partner),
           SOURCE, source_part)

    def project(index):
        unit = index // depth
        level = index % depth
        with jax.named_scope("project"):
            block = sbuf[unit].reshape(rows, width)
            start = pl.multiple_of(unit * rows, rows)
            k = jnp.dot(block, wk[level], preferred_element_type=F32)
            keys[level, pl.ds(start, rows), :] = k.astype(BF16)
            v = jnp.dot(block, wv[level], preferred_element_type=F32)
            values[level, pl.ds(start, rows), :] = v.astype(BF16)

    def project_half(unit, level, part):
        with jax.named_scope("project_half"):
            block = sbuf[unit, :, pl.ds(part * (half // 2), half // 2)].reshape(half, width)
            start = pl.multiple_of(unit * rows + part * half, half)
            k = jnp.dot(block, wk[level], preferred_element_type=F32)
            keys[level, pl.ds(start, half), :] = k.astype(BF16)
            v = jnp.dot(block, wv[level], preferred_element_type=F32)
            values[level, pl.ds(start, half), :] = v.astype(BF16)

    def query_copy(level, p, block, j):
        sem = first_recv.at[0] if level == 0 else q_recv.at[level - 1, p, block]
        rows_of = qbuf.at[level, p, block]
        return remote(rows_of, rows_of, send_sem.at[LINE], sem, {"sp": j})

    def forward(level, p):
        @pl.when(inner)
        def _():
            for block in (far_inner, far_edge):
                arrived(q_recv.at[level - 1, p, block], result_block)
                query_copy(level, p, block, near).start()

    def send_queries(level, p):
        if level == 0:
            query_copy(level, p, s, far_edge).start()
        query_copy(level, p, s, far_inner).start()
        if level == 0 or p == 0:
            query_copy(level, p, s, near).start()
        else:
            @pl.when(edge)
            def _():
                query_copy(level, p, s, near).start()

    def drain_line():
        def drain(queries):
            blocks = PIECES * ((depth + 1) * (sp - 1) + (depth - 1) * queries)
            arrived(send_sem.at[LINE], *([result_block] * blocks),
                    *([stats_block] * (depth * PIECES * (sp - 1))))

        @pl.when(edge)
        def _():
            drain(2)

        @pl.when(inner)
        def _():
            drain(4)

    def send_result(level, p, j):
        remote(osend.at[level, p, j], orecv.at[level, p, s], send_sem.at[LINE],
               o_recv.at[level, p], {"sp": j}).start()
        remote(ssend.at[level, p, j], srecv.at[level, p, s], send_sem.at[LINE],
               o_recv.at[level, p], {"sp": j}).start()

    def send_aside(level, p):
        for slot, j in enumerate((far_edge, far_inner)):
            remote(osend.at[level, p, j], orelay.at[level, p, slot], send_sem.at[LINE],
                   m_recv.at[level, p, slot], {"sp": near}).start()
            remote(ssend.at[level, p, j], srelay.at[level, p, slot], send_sem.at[LINE],
                   m_recv.at[level, p, slot], {"sp": near}).start()

    def source_relay(unit, piece):
        span = pl.ds(*spans[piece])
        return remote(sbuf.at[unit, 0, span], sbuf.at[unit, 1, span], send_sem.at[SOURCE],
                      r_recv.at[unit - 2, min(piece, 1)], partner)

    def relay_pieces(unit, pieces):
        for piece in pieces:
            arrived(s_recv.at[unit - 2, piece], ((spans[piece][1], width), 2))
            source_relay(unit, piece).start()

    def first_queries():
        own_target.wait()
        own_gains.wait()
        for step in range(1, nx):
            slot = chip(step) * CORES + c
            arrived(t_recv.at[step], target_rows)
            go(remote(tbuf.at[slot], tbuf.at[slot], send_sem.at[SOURCE], t_recv.at[0], partner),
               SOURCE, target_rows)
        arrived(t_recv.at[0], *([target_rows] * nx))

        @pl.loop(0, tp)
        def _(block):
            value = tbuf[block].astype(F32)
            ready = normalize(value, gains[0, 0:1, :]).astype(BF16)
            for p in range(PIECES):
                span = slice(p * prows, (p + 1) * prows)
                stream[p, block] = value[span]
                normed[p, block] = ready[span]

        load(0, 0).wait()
        q = jnp.dot(normed[...].reshape(PIECES * piece_rows, width), wq[0],
                    preferred_element_type=F32)
        for p in range(PIECES):
            qbuf[0, p, s] = q[p * piece_rows:(p + 1) * piece_rows].astype(BF16)
            send_queries(0, p)

    @pl.loop(0, units * depth - (depth - 1))
    def _(index):
        unit = index // depth
        level = index % depth

        @pl.when(index == 0)
        def _():
            arrived(local_sem.at[1], source_part, source_part)
            arrived(weight_sem.at[1, 0], weight_block, weight_block)
            load(0, 0).start()
            for later in range(1, depth):
                load(1, later).start()
                load(2, later).start()
            load(3, 0).start()
            for later in range(1, depth):
                load(0, later).start()
                load(3, later).start()

        for later in range(1, depth):
            @pl.when(index == later)
            def _():
                arrived(weight_sem.at[1, later], weight_block, weight_block)

        @pl.when(index == depth)
        def _():
            with jax.named_scope("first_queries"):
                first_queries()
            arrived(p_recv.at[0], source_part, source_part)

        @pl.when(jnp.logical_and(unit >= 2, level == 0))
        def _():
            with jax.named_scope("wait_remote"):
                relay_pieces(unit, (0,))
                arrived(r_recv.at[unit - 2, 0], ((half // 2, width), 2))

            @pl.when(unit == units - 1)
            def _():
                project_half(unit, level, 0)

            with jax.named_scope("wait_remote2"):
                relay_pieces(unit, range(1, len(spans)))
            with jax.named_scope("wait_relayed"):
                arrived(r_recv.at[unit - 2, 1], ((half // 2, width), 2))

            @pl.when(unit == units - 1)
            def _():
                project_half(unit, level, 1)

        @pl.when(index < (units - 1) * depth)
        def _():
            project(index)

    sent[SOURCE] += [source_part] * (units - 2)
    arrived(first_recv.at[0], *([result_block] * (PIECES * (sp - 1))))

    def columns(parts):
        stacked = jnp.concatenate(parts, axis=0)
        fill = jnp.zeros((HEAD - stacked.shape[0], stacked.shape[1]), F32)
        return jnp.concatenate([stacked, fill], axis=0).T

    def weighted(cols, blocks, h):
        span = slice(h * HEAD, (h + 1) * HEAD)
        return sum(
            cols[0:piece_rows, k * heads + h:k * heads + h + 1] * block[:, span].astype(F32)
            for k, block in enumerate(blocks))

    def merge(layer, p):
        @pl.when(inner)
        def _():
            for slot, j in enumerate((far_edge, far_inner)):
                with jax.named_scope("merge_wait"):
                    arrived(m_recv.at[layer, p, slot], result_block, stats_block)
                with jax.named_scope("merge"):
                    mine, theirs = ssend[layer, p, j], srelay[layer, p, slot]
                    top = jnp.maximum(mine[0:heads], theirs[0:heads])
                    share = [jnp.exp2(one[0:heads] - top) for one in (mine, theirs)]
                    total = share[0] * mine[heads:] + share[1] * theirs[heads:]
                    cols = columns(share)
                    blocks = (osend[layer, p, j], orelay[layer, p, slot])
                    for h in range(heads):
                        osend[layer, p, j, :, h * HEAD:(h + 1) * HEAD] = weighted(
                            cols, blocks, h).astype(BF16)
                    ssend[layer, p, j] = jnp.concatenate([top, total], axis=0)
                    send_result(layer, p, j)

    def head_scores(layer, q, h):
        cols = slice(h * HEAD, (h + 1) * HEAD)
        scores = lax.dot_general(
            q[:, cols], keys[layer, :, cols], (((1,), (1,)), ((), ())), preferred_element_type=F32)
        return scores, jnp.max(scores, axis=1, keepdims=True) * score_scale

    def attend(layer, p, first, blocks):
        with jax.named_scope("attend"):
            count = blocks * piece_rows
            q = qbuf[layer, p, pl.ds(first, blocks)].reshape(count, local_width)
            lane = lax.broadcasted_iota(jnp.int32, (count, HEAD), 1)
            notes = jnp.zeros((count, HEAD), F32)
            ahead = head_scores(layer, q, 0)
            for h in range(heads):
                scores, peak = ahead
                if h + 1 < heads:
                    ahead = head_scores(layer, q, h + 1)
                cols = slice(h * HEAD, (h + 1) * HEAD)
                weights = jnp.exp2(scores * score_scale - peak)
                total = jnp.sum(weights, axis=1, keepdims=True)
                o = jnp.dot(weights.astype(BF16), values[layer, :, cols], preferred_element_type=F32)
                o = o.astype(BF16)
                for member in range(blocks):
                    osend[layer, p, first + member, :, cols] = o[member * piece_rows:(member + 1) * piece_rows]
                notes = jnp.where(lane == h, peak, notes)
                notes = jnp.where(lane == heads + h, total, notes)
            for two in range(blocks // 2):
                stats = notes[two * HEAD:(two + 1) * HEAD].T[0:2 * heads]
                ssend[layer, p, first + 2 * two] = stats
                ssend[layer, p, first + 2 * two + 1] = pltpu.roll(stats, piece_rows, 1)

    def keep_own(layer, p):
        orecv[layer, p, s] = osend[layer, p, s]
        srecv[layer, p, s] = ssend[layer, p, s]

    def out_project(layer, p):
        with jax.named_scope("wait_o"):
            arrived(o_recv.at[layer, p], *([result_block, stats_block] * 2))
        with jax.named_scope("combine_out"):
            origins = (s, near, far_inner)
            stats = [srecv[layer, p, j] for j in origins]
            top = functools.reduce(jnp.maximum, [one[0:heads] for one in stats])
            share = [jnp.exp2(one[0:heads] - top) for one in stats]
            total = sum(part * one[heads:] for part, one in zip(share, stats))
            cols = columns([part / total for part in share])
            blocks = [orecv[layer, p, j] for j in origins]
            for h in range(heads):
                attended[:, h * HEAD:(h + 1) * HEAD] = weighted(cols, blocks, h).astype(BF16)
            tile = min(512, width)
            for n in range(width // tile):
                span = slice(n * tile, (n + 1) * tile)
                part = jnp.dot(attended[...], wo[layer, :, span], preferred_element_type=F32).astype(BF16)
                for b in range(nx):
                    for core in range(CORES):
                        at = (b * CORES + core) * prows
                        pbuf[layer, p, core, b, :, span] = part[at:at + prows]
            go(remote(pbuf.at[layer, p, partner_c], half_in.at[layer, p], send_sem.at[ROW],
                      h_recv.at[layer, p], partner), ROW, chip_rows)

    def chip_total(layer, p):
        with jax.named_scope("chip_total"):
            arrived(h_recv.at[layer, p], chip_rows)
            for b in range(nx):
                both_cores = pbuf[layer, p, c, b].astype(F32) + half_in[layer, p, b].astype(F32)
                chip_sum[layer, p, x, c, b] = both_cores.astype(BF16)
            own = chip_sum.at[layer, p, x, c]
            for step in range(1, nx):
                go(remote(own, own, send_sem.at[ROW], c_recv.at[layer, p, nx - step - 1], peer(step)),
                   ROW, chip_rows)
            go(remote(own, own, send_sem.at[ROW], d_recv.at[layer, p], partner), ROW, chip_rows)

    def next_queries(layer, p):
        with jax.named_scope("xwait"):
            for step in range(1, nx):
                a = chip(step)
                other = chip_sum.at[layer, p, a, c]
                arrived(c_recv.at[layer, p, step - 1], chip_rows)
                go(remote(other, other, send_sem.at[ROW], d_recv.at[layer, p], partner), ROW, chip_rows)
            arrived(d_recv.at[layer, p], *([chip_rows] * nx))
        with jax.named_scope("norm_q"):
            for block in range(tp):
                projected = sum(
                    chip_sum[layer, p, a, block % CORES, block // CORES].astype(F32) for a in range(nx))
                value = stream[p, block] + normalize(projected, gains[layer, 1:2, :])
                stream[p, block] = value
                normed[p, block] = normalize(value, gains[layer + 1, 0:1, :]).astype(BF16)
            q = jnp.dot(normed[p].reshape(piece_rows, width), wq[layer + 1],
                        preferred_element_type=F32)
            qbuf[layer + 1, p, s] = q.astype(BF16)
            send_queries(layer + 1, p)

    def final_send(layer, p):
        with jax.named_scope("final_send"):
            arrived(h_recv.at[layer, p], chip_rows)
            for step in range(1, nx):
                b = chip(step)
                both_cores = pbuf[layer, p, c, b].astype(F32) + half_in[layer, p, b].astype(F32)
                fin[0, p, b] = both_cores.astype(BF16)
                go(remote(fin.at[0, p, b], fin.at[1, p, x], send_sem.at[ROW],
                          f_recv.at[p, nx - step - 1], peer(step)), ROW, sum_block)

    def final_rows(layer, p):
        with jax.named_scope("final_rows"):
            projected = pbuf[layer, p, c, x].astype(F32) + half_in[layer, p, x].astype(F32)
            for step in range(1, nx):
                b = chip(step)
                arrived(f_recv.at[p, step - 1], sum_block)
                projected = projected + fin[1, p, b].astype(F32)
            value = stream[p, t] + normalize(projected, gains[layer, 1:2, :])
            out[p * prows:(p + 1) * prows, :] = value.astype(out.dtype)

    for layer in range(depth):
        last = layer == depth - 1
        own_pair = s // 2
        if layer == 1:
            @pl.loop(units * depth - (depth - 1), units * depth)
            def _(index):
                project(index)

        if layer == 0:
            @pl.loop(0, 2 * PIECES)
            def _(i):
                p, far = i % PIECES, i < PIECES
                attend(layer, p, jnp.where(far, 2 * (1 - own_pair), 2 * own_pair), 2)

                @pl.when(jnp.logical_and(edge, far))
                def _():
                    send_aside(layer, p)

                @pl.when(jnp.logical_not(far))
                def _():
                    send_result(layer, p, near)
                    keep_own(layer, p)
        else:
            @pl.loop(0, 2 * PIECES)
            def _(i):
                p, close = i // 2, i % 2 == 0

                @pl.when(close)
                def _():
                    forward(layer, p)

                    @pl.when(jnp.logical_and(inner, p + 1 < PIECES))
                    def _():
                        query_copy(layer, p + 1, s, near).start()

                    with jax.named_scope("wait_near"):
                        arrived(q_recv.at[layer - 1, p, near], result_block)

                @pl.when(jnp.logical_and(edge, jnp.logical_not(close)))
                def _():
                    with jax.named_scope("wait_far"):
                        for block in (far_inner, far_edge):
                            arrived(q_recv.at[layer - 1, p, block], result_block)

                attend(layer, p, jnp.where(close, 2 * own_pair, 2 * (1 - own_pair)), 2)

                @pl.when(close)
                def _():
                    keep_own(layer, p)

                @pl.when(jnp.logical_and(edge, close))
                def _():
                    send_result(layer, p, near)

                @pl.when(jnp.logical_and(inner, i == 2 * PIECES - 2))
                def _():
                    for later in range(PIECES):
                        send_result(layer, later, near)

                @pl.when(jnp.logical_and(edge, jnp.logical_not(close)))
                def _():
                    send_aside(layer, p)

        total = final_send if last else chip_total
        load(3, layer).wait()
        for p in range(PIECES):
            merge(layer, p)
        for p in range(PIECES):
            out_project(layer, p)
            total(layer, p)
        if not last:
            load(0, layer + 1).wait()
        for p in range(PIECES):
            if last:
                final_rows(layer, p)
            else:
                next_queries(layer, p)

    with jax.named_scope("finish"):
        drain_line()
        for kind in (SOURCE, ROW):
            arrived(send_sem.at[kind], *sent[kind])


def fused_body(nx, sp, target, source, w_query, w_key, w_value, w_out, gains):
    depth, width, local_width = w_query.shape
    trows, rows = target.shape[0], source.shape[0]
    tp = nx * CORES
    prows = trows // PIECES
    piece_rows = tp * prows
    heads = local_width // HEAD
    units = 2 * nx
    vmem = pltpu.VMEM
    dma = pltpu.SemaphoreType.DMA
    anywhere = pl.BlockSpec(memory_space=pl.ANY)
    whole = pl.BlockSpec(memory_space=pltpu.VMEM)
    results = (depth, PIECES, sp, piece_rows, local_width)
    notes = (depth, PIECES, sp, 2 * heads, 2 * piece_rows)
    return pl.pallas_call(
        functools.partial(fused_kernel, nx, sp, depth),
        out_shape=jax.ShapeDtypeStruct((trows, width), BF16),
        in_specs=[anywhere] * 7,
        out_specs=whole,
        scratch_shapes=[
            vmem((tp, trows, width), BF16),
            vmem((units, 2, rows // 2, width), BF16),
            vmem(w_query.shape, BF16),
            vmem(w_key.shape, BF16),
            vmem(w_value.shape, BF16),
            vmem(w_out.shape, BF16),
            vmem((depth, units * rows, local_width), BF16),
            vmem((depth, units * rows, local_width), BF16),
            vmem((PIECES, tp, prows, width), F32),
            vmem((PIECES, tp, prows, width), BF16),
            vmem(results, BF16),
            vmem(results, BF16),
            vmem(results, BF16),
            vmem(notes, F32),
            vmem(notes, F32),
            vmem(results[:2] + (2,) + results[3:], BF16),
            vmem(notes[:2] + (2,) + notes[3:], F32),
            vmem((piece_rows, local_width), BF16),
            vmem((depth, PIECES, CORES, nx, prows, width), BF16),
            vmem((depth, PIECES, nx, prows, width), BF16),
            vmem((depth, PIECES, nx, CORES, nx, prows, width), BF16),
            vmem((2, PIECES, nx, prows, width), BF16),
            vmem((1024, 8, 128), F32),
            vmem(gains.shape, F32),
            dma((3,)), dma((3, depth)), dma((3,)), dma((nx,)),
            dma((units - 2, 4)), dma((1,)), dma((units - 2, 2)), dma((1,)), dma((depth - 1, PIECES, sp)),
            dma((depth, PIECES)), dma((depth, PIECES, 2)), dma((depth, PIECES)),
            dma((depth - 1, PIECES, nx - 1)), dma((depth - 1, PIECES)), dma((PIECES, nx - 1)),
        ],
        compiler_params=pltpu.CompilerParams(
            collective_id=0, has_side_effects=True, vmem_limit_bytes=VMEM_KIB * 1024),
    )(*[pltpu.with_memory_space_constraint(one, pltpu.HBM) for one in (
        target, source, w_query, w_key, w_value, w_out, gains)])


def split_heads(row_block):
    return row_block.reshape(row_block.shape[0], row_block.shape[1] // HEAD, HEAD)


def body(target, source, w_query, w_key, w_value, w_out, gains):
    local_width = w_query.shape[2]
    score_scale = HEAD ** (-0.5)
    depth = w_query.shape[0]
    project_shard_part = lax.all_gather(source, "tp", axis=0, tiled=True)
    layer_parts = [
        jnp.stack(
            [
                jnp.dot(project_shard_part, w_key[level], preferred_element_type=jnp.float32),
                jnp.dot(project_shard_part, w_value[level], preferred_element_type=jnp.float32),
            ]
        )
        for level in range(depth)
    ]
    projected_source = jnp.stack(layer_parts).astype(jnp.bfloat16)
    stream = target.astype(jnp.float32)
    for layer_index in range(depth):
        normed = normalize(stream, gains[layer_index, 0]).astype(jnp.bfloat16)
        query_weight = w_query[layer_index]
        queries = jnp.dot(
            lax.all_gather(normed, "tp", axis=0, tiled=True),
            query_weight,
            preferred_element_type=jnp.float32,
        ).astype(jnp.bfloat16)
        row_count = queries.shape[0]
        keys_here = projected_source[layer_index, 0]
        values_here = projected_source[layer_index, 1]
        every_query = lax.all_gather(queries, "sp", axis=0, tiled=True)
        scores = (
            jnp.einsum(
                "qhd,khd->hqk",
                split_heads(every_query),
                split_heads(keys_here),
                preferred_element_type=jnp.float32,
            )
            * score_scale
        )
        row_peak = lax.pmax(jnp.max(scores, axis=2), "sp")
        weights = jnp.exp(scores - row_peak[:, :, None])
        local_summed = jnp.einsum(
            "hqk,khd->hqd",
            weights.astype(jnp.bfloat16),
            split_heads(values_here),
            preferred_element_type=jnp.float32,
        )
        summed, row_total = (
            lax.psum_scatter(
                local_summed.astype(jnp.bfloat16), "sp", scatter_dimension=1, tiled=True
            ).astype(jnp.float32),
            lax.psum_scatter(
                jnp.sum(weights, axis=2).astype(jnp.bfloat16), "sp", scatter_dimension=1, tiled=True
            ).astype(jnp.float32),
        )
        heads_out = summed / row_total[:, :, None]
        attended = (
            jnp.transpose(heads_out, (1, 0, 2)).reshape(row_count, local_width).astype(jnp.bfloat16)
        )
        out_weight = w_out[layer_index]
        projected = lax.psum_scatter(
            jnp.dot(attended, out_weight, preferred_element_type=jnp.float32).astype(jnp.bfloat16),
            "tp",
            scatter_dimension=0,
            tiled=True,
        ).astype(jnp.float32)
        stream = stream + normalize(projected, gains[layer_index, 1])
    return stream.astype(jnp.bfloat16)


def solution(mesh):
    in_specs = (
        P(("grp", "sp", "tp"), None),
        P(("grp", "sp", "tp"), None),
        P(None, None, "tp"),
        P(None, None, "tp"),
        P(None, None, "tp"),
        P(None, "tp", None),
        P(),
    )
    out_specs = P(("grp", "sp", "tp"), None)
    sp, tp = mesh.shape["sp"], mesh.shape["tp"]

    def run(target, source, w_query, w_key, w_value, w_out, gains):
        trows, rows, local_width = target.shape[0], source.shape[0], w_query.shape[2]
        tiles = (trows % (16 * PIECES) == 0 and tp * trows == PIECES * (HEAD // 2) and rows % 128 == 0
                 and sp % 2 == 0 and sp // 2 == 2 and w_query.shape[0] > 1 and tp > CORES
                 and local_width % (4 * HEAD) == 0 and tp % CORES == 0)
        form = functools.partial(fused_body, tp // CORES, sp) if tiles else body
        return form(target, source, w_query, w_key, w_value, w_out, gains)

    return jax.shard_map(run, mesh=mesh, in_specs=in_specs, out_specs=out_specs, check_vma=False)
```

```python
import functools
import math

import jax
import jax.numpy as jnp
from jax import lax
from jax.experimental import pallas as pl
from jax.experimental.pallas import tpu as pltpu
from jax.sharding import PartitionSpec as P

HEAD = 128
CORES = 2
PIECES = 2
SWAPPED = 2
VMEM_KIB = 50000


EPS = 1e-06
MESH = pl.DeviceIdType.MESH
F32 = jnp.float32
BF16 = jnp.bfloat16


def normalize(row_block, gain_row):
    return (
        row_block
        * lax.rsqrt(jnp.mean(row_block * row_block, axis=-1, keepdims=True) + EPS)
        * gain_row
    )


def fused_kernel(
    nx, sp, depth,
    target, source, w_query, w_key, w_value, w_out, gain_rows, out,
    tbuf, sbuf, wq, wk, wv, wo, keys, values, stream, normed, qbuf,
    osend, orecv, ssend, srecv, orelay, srelay, attended, pbuf, half_in, chip_sum, fin, ledger, gains,
    local_sem, weight_sem, send_sem, t_recv, s_recv, p_recv, r_recv, first_recv, q_recv,
    x_recv, o_recv, m_recv, h_recv, c_recv, d_recv, f_recv,
):
    s = lax.axis_index("sp")
    t = lax.axis_index("tp")
    x = t // CORES
    c = t % CORES
    partner_c = 1 - c
    partner = {"tp": x * CORES + partner_c}
    units = sbuf.shape[0]
    half = sbuf.shape[2]
    width = sbuf.shape[3]
    rows = 2 * half
    local_width = wk.shape[2]
    heads = local_width // HEAD
    tp = nx * CORES
    prows = stream.shape[2]
    piece_rows = tp * prows
    score_scale = HEAD ** (-0.5) * math.log2(math.e)

    pairs = sp // 2
    edge = jnp.logical_or(s == 0, s == sp - 1)
    inner = jnp.logical_not(edge)
    low = s < pairs
    near = jnp.where(s % 2 == 0, s + 1, s - 1)
    far_edge = jnp.where(low, sp - 1, 0)
    far_inner = jnp.where(low, pairs, pairs - 1)

    def chip(step):
        return lax.rem(x + step, nx)

    def peer(step):
        return {"tp": chip(step) * CORES + c}

    def remote(src, dst, send_sem, recv_sem, device):
        return pltpu.make_async_remote_copy(
            src_ref=src, dst_ref=dst, send_sem=send_sem, recv_sem=recv_sem,
            device_id=device, device_id_type=MESH,
        )

    def arrived(sem, *shapes):
        total = sum(math.prod(shape) * size for shape, size in shapes)
        block = ledger.at[pl.ds(0, total // math.prod(ledger.shape[1:]) // 4)]
        pltpu.make_async_copy(block, block, sem).wait()

    target_rows = (tbuf.shape[1:], 2)
    source_part = (sbuf.shape[2:], 2)
    result_block = (osend.shape[3:], 2)
    stats_block = (ssend.shape[3:], 4)
    sum_block = (half_in.shape[3:], 2)
    chip_rows = (half_in.shape[2:], 2)
    weight_block = (wk.shape[1:], 2)

    own_target = pltpu.make_async_copy(target, tbuf.at[t], local_sem.at[0])
    own_source = [
        pltpu.make_async_copy(
            source.at[pl.ds(part * half, half)], sbuf.at[0, part], local_sem.at[1])
        for part in range(2)
    ]

    def load(kind, level):
        pair = ((w_query, wq), (w_key, wk), (w_value, wv), (w_out, wo))[kind]
        return pltpu.make_async_copy(
            pair[0].at[level], pair[1].at[level], weight_sem.at[(0, 1, 1, 2)[kind], level])

    own_gains = pltpu.make_async_copy(gain_rows, gains, local_sem.at[2])
    own_target.start()
    own_gains.start()
    for copy in own_source:
        copy.start()
    load(1, 0).start()
    load(2, 0).start()

    barrier = pltpu.get_barrier_semaphore()
    pl.semaphore_signal(barrier, inc=1, device_id=partner, device_id_type=MESH)
    for step in range(1, nx):
        pl.semaphore_signal(barrier, inc=1, device_id=peer(step), device_id_type=MESH)
        pl.semaphore_signal(
            barrier, inc=1, device_id={"tp": chip(step) * CORES + partner_c}, device_id_type=MESH)
    for step in range(1, sp):
        pl.semaphore_signal(
            barrier, inc=1, device_id={"sp": lax.rem(s + step, sp)}, device_id_type=MESH)
    with jax.named_scope("barrier"):
        pl.semaphore_wait(barrier, 1 + 2 * (nx - 1) + (sp - 1))

    spans = ((0, half // 2), (half // 2, half // 4), (3 * half // 4, half // 8), (7 * half // 8, half // 8))
    swapped_rows = half - spans[SWAPPED][0]
    SOURCE, LINE, ROW = range(3)
    sent = {SOURCE: [], LINE: [], ROW: []}

    def go(copy, kind, shape):
        copy.start()
        sent[kind].append(shape)

    for step in range(1, nx):
        go(remote(target, tbuf.at[t], send_sem.at[SOURCE], t_recv.at[step], peer(step)),
           SOURCE, target_rows)
    go(remote(target, tbuf.at[t], send_sem.at[SOURCE], t_recv.at[0], partner), SOURCE, target_rows)
    for part in range(2):
        block = source.at[pl.ds(part * half, half)]
        for piece, (at, size) in enumerate(spans):
            span = pl.ds(at, size)
            for step in range(1, nx):
                unit = 2 * (nx - step) + part
                copy = remote(block.at[span], sbuf.at[unit, 0, span], send_sem.at[SOURCE],
                              s_recv.at[unit - 2, piece], peer(step))
                if part == 1 and piece >= SWAPPED:
                    pl.when(c == 1)(copy.start)
                    sent[SOURCE].append(((size, width), 2))

                    @pl.when(c == 0)
                    def _():
                        remote(block.at[span], sbuf.at[unit, 1, span], send_sem.at[SOURCE],
                               x_recv.at[nx - step - 1, piece - SWAPPED],
                               {"tp": chip(step) * CORES + 1}).start()
                else:
                    go(copy, SOURCE, ((size, width), 2))
        go(remote(block, sbuf.at[1, part], send_sem.at[SOURCE], p_recv.at[0], partner),
           SOURCE, source_part)

    def project(index):
        unit = index // depth
        level = index % depth
        with jax.named_scope("project"):
            block = sbuf[unit].reshape(rows, width)
            start = pl.multiple_of(unit * rows, rows)
            k = jnp.dot(block, wk[level], preferred_element_type=F32)
            keys[level, pl.ds(start, rows), :] = k.astype(BF16)
            v = jnp.dot(block, wv[level], preferred_element_type=F32)
            values[level, pl.ds(start, rows), :] = v.astype(BF16)

    def project_half(unit, level, part):
        with jax.named_scope("project_half"):
            block = sbuf[unit, :, pl.ds(part * (half // 2), half // 2)].reshape(half, width)
            start = pl.multiple_of(unit * rows + part * half, half)
            k = jnp.dot(block, wk[level], preferred_element_type=F32)
            keys[level, pl.ds(start, half), :] = k.astype(BF16)
            v = jnp.dot(block, wv[level], preferred_element_type=F32)
            values[level, pl.ds(start, half), :] = v.astype(BF16)

    def query_copy(level, p, block, j):
        sem = first_recv.at[0] if level == 0 else q_recv.at[level - 1, p, block]
        rows_of = qbuf.at[level, p, block]
        return remote(rows_of, rows_of, send_sem.at[LINE], sem, {"sp": j})

    def forward(level, p):
        @pl.when(inner)
        def _():
            for block in (far_inner, far_edge):
                arrived(q_recv.at[level - 1, p, block], result_block)
                query_copy(level, p, block, near).start()

    def hand_on(level, p):
        forward(level, p)

        @pl.when(jnp.logical_and(inner, p + 1 < PIECES))
        def _():
            query_copy(level, p + 1, s, near).start()

    def send_queries(level, p):
        if level == 0:
            query_copy(level, p, s, far_edge).start()
        query_copy(level, p, s, far_inner).start()
        if level == 0 or p == 0:
            query_copy(level, p, s, near).start()
        else:
            @pl.when(edge)
            def _():
                query_copy(level, p, s, near).start()

    def drain_line():
        def drain(queries):
            blocks = PIECES * ((depth + 1) * (sp - 1) + (depth - 1) * queries)
            arrived(send_sem.at[LINE], *([result_block] * blocks),
                    *([stats_block] * (depth * PIECES * (sp - 1))))

        @pl.when(edge)
        def _():
            drain(2)

        @pl.when(inner)
        def _():
            drain(4)

    def send_result(level, p, j):
        remote(osend.at[level, p, j], orecv.at[level, p, s], send_sem.at[LINE],
               o_recv.at[level, p], {"sp": j}).start()
        remote(ssend.at[level, p, j], srecv.at[level, p, s], send_sem.at[LINE],
               o_recv.at[level, p], {"sp": j}).start()

    def send_aside(level, p):
        for slot, j in enumerate((far_edge, far_inner)):
            remote(osend.at[level, p, j], orelay.at[level, p, slot], send_sem.at[LINE],
                   m_recv.at[level, p, slot], {"sp": near}).start()
            remote(ssend.at[level, p, j], srelay.at[level, p, slot], send_sem.at[LINE],
                   m_recv.at[level, p, slot], {"sp": near}).start()

    def source_relay(unit, piece):
        span = pl.ds(*spans[piece])
        return remote(sbuf.at[unit, 0, span], sbuf.at[unit, 1, span], send_sem.at[SOURCE],
                      r_recv.at[unit - 2, min(piece, 1)], partner)

    def relay_pieces(unit, pieces):
        for piece in pieces:
            arrived(s_recv.at[unit - 2, piece], ((spans[piece][1], width), 2))
            source_relay(unit, piece).start()

    def first_queries():
        own_target.wait()
        own_gains.wait()
        for step in range(1, nx):
            slot = chip(step) * CORES + c
            arrived(t_recv.at[step], target_rows)
            go(remote(tbuf.at[slot], tbuf.at[slot], send_sem.at[SOURCE], t_recv.at[0], partner),
               SOURCE, target_rows)
        arrived(t_recv.at[0], *([target_rows] * nx))

        @pl.loop(0, tp)
        def _(block):
            value = tbuf[block].astype(F32)
            ready = normalize(value, gains[0, 0:1, :]).astype(BF16)
            for p in range(PIECES):
                span = slice(p * prows, (p + 1) * prows)
                stream[p, block] = value[span]
                normed[p, block] = ready[span]

        load(0, 0).wait()
        q = jnp.dot(normed[...].reshape(PIECES * piece_rows, width), wq[0],
                    preferred_element_type=F32)
        for p in range(PIECES):
            qbuf[0, p, s] = q[p * piece_rows:(p + 1) * piece_rows].astype(BF16)
            send_queries(0, p)

    @pl.loop(0, units * depth - (depth - 1))
    def _(index):
        unit = index // depth
        level = index % depth

        @pl.when(index == 0)
        def _():
            arrived(local_sem.at[1], source_part, source_part)
            arrived(weight_sem.at[1, 0], weight_block, weight_block)
            load(0, 0).start()
            for later in range(1, depth):
                load(1, later).start()
                load(2, later).start()
            load(3, 0).start()
            for later in range(1, depth):
                load(0, later).start()
                load(3, later).start()

        for later in range(1, depth):
            @pl.when(index == later)
            def _():
                arrived(weight_sem.at[1, later], weight_block, weight_block)

        @pl.when(index == depth)
        def _():
            with jax.named_scope("first_queries"):
                first_queries()
            arrived(p_recv.at[0], source_part, source_part)

        @pl.when(jnp.logical_and(unit >= 2, level == 0))
        def _():
            with jax.named_scope("wait_remote"):
                relay_pieces(unit, (0,))
                arrived(r_recv.at[unit - 2, 0], ((half // 2, width), 2))

            @pl.when(unit == units - 1)
            def _():
                project_half(unit, level, 0)

            with jax.named_scope("wait_remote2"):
                relay_pieces(unit, range(1, SWAPPED))
                shared = unit % 2 == 1

                @pl.when(jnp.logical_or(c == 1, jnp.logical_not(shared)))
                def _():
                    relay_pieces(unit, range(SWAPPED, len(spans)))

                @pl.when(jnp.logical_and(c == 1, shared))
                def _():
                    for piece in range(SWAPPED, len(spans)):
                        span = pl.ds(*spans[piece])
                        arrived(x_recv.at[(unit - 3) // 2, piece - SWAPPED], ((spans[piece][1], width), 2))
                        remote(sbuf.at[unit, 1, span], sbuf.at[unit, 0, span], send_sem.at[SOURCE],
                               r_recv.at[unit - 2, 1], partner).start()

            with jax.named_scope("wait_relayed"):
                @pl.when(jnp.logical_not(shared))
                def _():
                    arrived(r_recv.at[unit - 2, 1], ((half // 2, width), 2))

                @pl.when(jnp.logical_and(c == 0, shared))
                def _():
                    arrived(r_recv.at[unit - 2, 1], ((half // 2 + swapped_rows, width), 2))

                @pl.when(jnp.logical_and(c == 1, shared))
                def _():
                    arrived(r_recv.at[unit - 2, 1], ((half // 2 - swapped_rows, width), 2))

            @pl.when(unit == units - 1)
            def _():
                project_half(unit, level, 1)

        @pl.when(index < (units - 1) * depth)
        def _():
            project(index)

    sent[SOURCE] += [source_part] * (units - 2 - (nx - 1))
    sent[SOURCE] += [((half - swapped_rows, width), 2)] * (nx - 1)
    arrived(first_recv.at[0], *([result_block] * (PIECES * (sp - 1))))

    def columns(parts):
        stacked = jnp.concatenate(parts, axis=0)
        fill = jnp.zeros((HEAD - stacked.shape[0], stacked.shape[1]), F32)
        return jnp.concatenate([stacked, fill], axis=0).T

    def weighted(cols, blocks, h):
        span = slice(h * HEAD, (h + 1) * HEAD)
        return sum(
            cols[0:piece_rows, k * heads + h:k * heads + h + 1] * block[:, span].astype(F32)
            for k, block in enumerate(blocks))

    def merge(layer, p):
        @pl.when(inner)
        def _():
            for slot, j in enumerate((far_edge, far_inner)):
                with jax.named_scope("merge_wait"):
                    arrived(m_recv.at[layer, p, slot], result_block, stats_block)
                with jax.named_scope("merge"):
                    mine, theirs = ssend[layer, p, j], srelay[layer, p, slot]
                    top = jnp.maximum(mine[0:heads], theirs[0:heads])
                    share = [jnp.exp2(one[0:heads] - top) for one in (mine, theirs)]
                    total = share[0] * mine[heads:] + share[1] * theirs[heads:]
                    cols = columns(share)
                    blocks = (osend[layer, p, j], orelay[layer, p, slot])
                    for h in range(heads):
                        osend[layer, p, j, :, h * HEAD:(h + 1) * HEAD] = weighted(
                            cols, blocks, h).astype(BF16)
                    ssend[layer, p, j] = jnp.concatenate([top, total], axis=0)
                    send_result(layer, p, j)

    def head_scores(layer, q, h):
        cols = slice(h * HEAD, (h + 1) * HEAD)
        scores = lax.dot_general(
            q[:, cols], keys[layer, :, cols], (((1,), (1,)), ((), ())), preferred_element_type=F32)
        return scores, jnp.max(scores, axis=1, keepdims=True) * score_scale

    def attend(layer, p, first, blocks):
        with jax.named_scope("attend"):
            count = blocks * piece_rows
            q = qbuf[layer, p, pl.ds(first, blocks)].reshape(count, local_width)
            lane = lax.broadcasted_iota(jnp.int32, (count, HEAD), 1)
            notes = jnp.zeros((count, HEAD), F32)
            ahead = head_scores(layer, q, 0)
            for h in range(heads):
                scores, peak = ahead
                if h + 1 < heads:
                    ahead = head_scores(layer, q, h + 1)
                cols = slice(h * HEAD, (h + 1) * HEAD)
                weights = jnp.exp2(scores * score_scale - peak)
                total = jnp.sum(weights, axis=1, keepdims=True)
                o = jnp.dot(weights.astype(BF16), values[layer, :, cols], preferred_element_type=F32)
                o = o.astype(BF16)
                for member in range(blocks):
                    osend[layer, p, first + member, :, cols] = o[member * piece_rows:(member + 1) * piece_rows]
                notes = jnp.where(lane == h, peak, notes)
                notes = jnp.where(lane == heads + h, total, notes)
            for two in range(blocks // 2):
                stats = notes[two * HEAD:(two + 1) * HEAD].T[0:2 * heads]
                ssend[layer, p, first + 2 * two] = stats
                ssend[layer, p, first + 2 * two + 1] = pltpu.roll(stats, piece_rows, 1)

    def keep_own(layer, p):
        orecv[layer, p, s] = osend[layer, p, s]
        srecv[layer, p, s] = ssend[layer, p, s]

    def out_project(layer, p):
        with jax.named_scope("wait_o"):
            arrived(o_recv.at[layer, p], *([result_block, stats_block] * 2))
        with jax.named_scope("combine_out"):
            origins = (s, near, far_inner)
            stats = [srecv[layer, p, j] for j in origins]
            top = functools.reduce(jnp.maximum, [one[0:heads] for one in stats])
            share = [jnp.exp2(one[0:heads] - top) for one in stats]
            total = sum(part * one[heads:] for part, one in zip(share, stats))
            cols = columns([part / total for part in share])
            blocks = [orecv[layer, p, j] for j in origins]
            for h in range(heads):
                attended[:, h * HEAD:(h + 1) * HEAD] = weighted(cols, blocks, h).astype(BF16)
            tile = min(512, width)
            for n in range(width // tile):
                span = slice(n * tile, (n + 1) * tile)
                part = jnp.dot(attended[...], wo[layer, :, span], preferred_element_type=F32).astype(BF16)
                for b in range(nx):
                    for core in range(CORES):
                        at = (b * CORES + core) * prows
                        pbuf[layer, p, core, b, :, span] = part[at:at + prows]
            go(remote(pbuf.at[layer, p, partner_c], half_in.at[layer, p], send_sem.at[ROW],
                      h_recv.at[layer, p], partner), ROW, chip_rows)

    def chip_total(layer, p):
        with jax.named_scope("chip_total"):
            arrived(h_recv.at[layer, p], chip_rows)
            for b in range(nx):
                both_cores = pbuf[layer, p, c, b].astype(F32) + half_in[layer, p, b].astype(F32)
                chip_sum[layer, p, x, c, b] = both_cores.astype(BF16)
            own = chip_sum.at[layer, p, x, c]
            for step in range(1, nx):
                go(remote(own, own, send_sem.at[ROW], c_recv.at[layer, p, nx - step - 1], peer(step)),
                   ROW, chip_rows)
            go(remote(own, own, send_sem.at[ROW], d_recv.at[layer, p], partner), ROW, chip_rows)

    def next_queries(layer, p):
        with jax.named_scope("xwait"):
            for step in range(1, nx):
                a = chip(step)
                other = chip_sum.at[layer, p, a, c]
                arrived(c_recv.at[layer, p, step - 1], chip_rows)
                go(remote(other, other, send_sem.at[ROW], d_recv.at[layer, p], partner), ROW, chip_rows)
            arrived(d_recv.at[layer, p], *([chip_rows] * nx))
        with jax.named_scope("norm_q"):
            for block in range(tp):
                projected = sum(
                    chip_sum[layer, p, a, block % CORES, block // CORES].astype(F32) for a in range(nx))
                value = stream[p, block] + normalize(projected, gains[layer, 1:2, :])
                stream[p, block] = value
                normed[p, block] = normalize(value, gains[layer + 1, 0:1, :]).astype(BF16)
            q = jnp.dot(normed[p].reshape(piece_rows, width), wq[layer + 1],
                        preferred_element_type=F32)
            qbuf[layer + 1, p, s] = q.astype(BF16)
            send_queries(layer + 1, p)

    def final_send(layer, p):
        with jax.named_scope("final_send"):
            arrived(h_recv.at[layer, p], chip_rows)
            for step in range(1, nx):
                b = chip(step)
                both_cores = pbuf[layer, p, c, b].astype(F32) + half_in[layer, p, b].astype(F32)
                fin[0, p, b] = both_cores.astype(BF16)
                go(remote(fin.at[0, p, b], fin.at[1, p, x], send_sem.at[ROW],
                          f_recv.at[p, nx - step - 1], peer(step)), ROW, sum_block)

    def final_rows(layer, p):
        with jax.named_scope("final_rows"):
            projected = pbuf[layer, p, c, x].astype(F32) + half_in[layer, p, x].astype(F32)
            for step in range(1, nx):
                b = chip(step)
                arrived(f_recv.at[p, step - 1], sum_block)
                projected = projected + fin[1, p, b].astype(F32)
            value = stream[p, t] + normalize(projected, gains[layer, 1:2, :])
            out[p * prows:(p + 1) * prows, :] = value.astype(out.dtype)

    for layer in range(depth):
        last = layer == depth - 1
        own_pair = s // 2
        if layer > 0:
            hand_on(layer, 0)
        if layer == 1:
            @pl.loop(units * depth - (depth - 1), units * depth)
            def _(index):
                project(index)

        if layer == 0:
            @pl.loop(0, 2 * PIECES)
            def _(i):
                p, far = i % PIECES, i < PIECES
                attend(layer, p, jnp.where(far, 2 * (1 - own_pair), 2 * own_pair), 2)

                @pl.when(jnp.logical_and(edge, far))
                def _():
                    send_aside(layer, p)

                @pl.when(jnp.logical_not(far))
                def _():
                    send_result(layer, p, near)
                    keep_own(layer, p)
        else:
            @pl.loop(0, 2 * PIECES)
            def _(i):
                p, close = i // 2, i % 2 == 0

                @pl.when(close)
                def _():
                    @pl.when(p > 0)
                    def _():
                        hand_on(layer, p)

                    with jax.named_scope("wait_near"):
                        arrived(q_recv.at[layer - 1, p, near], result_block)

                @pl.when(jnp.logical_and(edge, jnp.logical_not(close)))
                def _():
                    with jax.named_scope("wait_far"):
                        for block in (far_inner, far_edge):
                            arrived(q_recv.at[layer - 1, p, block], result_block)

                attend(layer, p, jnp.where(close, 2 * own_pair, 2 * (1 - own_pair)), 2)

                @pl.when(close)
                def _():
                    keep_own(layer, p)

                @pl.when(jnp.logical_and(edge, close))
                def _():
                    send_result(layer, p, near)

                @pl.when(jnp.logical_and(inner, i == 2 * PIECES - 2))
                def _():
                    for later in range(PIECES):
                        send_result(layer, later, near)

                @pl.when(jnp.logical_and(edge, jnp.logical_not(close)))
                def _():
                    send_aside(layer, p)

        total = final_send if last else chip_total
        load(3, layer).wait()
        for p in range(PIECES):
            merge(layer, p)
        for p in range(PIECES):
            out_project(layer, p)
            total(layer, p)
        if not last:
            load(0, layer + 1).wait()
        for p in range(PIECES):
            if last:
                final_rows(layer, p)
            else:
                next_queries(layer, p)

    with jax.named_scope("finish"):
        drain_line()
        arrived(send_sem.at[ROW], *sent[ROW])
        moved = ((swapped_rows * (nx - 1), width), 2)

        @pl.when(c == 0)
        def _():
            arrived(send_sem.at[SOURCE], *sent[SOURCE])

        @pl.when(c == 1)
        def _():
            arrived(send_sem.at[SOURCE], *sent[SOURCE], moved, moved)


def fused_body(nx, sp, target, source, w_query, w_key, w_value, w_out, gains):
    depth, width, local_width = w_query.shape
    trows, rows = target.shape[0], source.shape[0]
    tp = nx * CORES
    prows = trows // PIECES
    piece_rows = tp * prows
    heads = local_width // HEAD
    units = 2 * nx
    vmem = pltpu.VMEM
    dma = pltpu.SemaphoreType.DMA
    anywhere = pl.BlockSpec(memory_space=pl.ANY)
    whole = pl.BlockSpec(memory_space=pltpu.VMEM)
    results = (depth, PIECES, sp, piece_rows, local_width)
    notes = (depth, PIECES, sp, 2 * heads, 2 * piece_rows)
    return pl.pallas_call(
        functools.partial(fused_kernel, nx, sp, depth),
        out_shape=jax.ShapeDtypeStruct((trows, width), BF16),
        in_specs=[anywhere] * 7,
        out_specs=whole,
        scratch_shapes=[
            vmem((tp, trows, width), BF16),
            vmem((units, 2, rows // 2, width), BF16),
            vmem(w_query.shape, BF16),
            vmem(w_key.shape, BF16),
            vmem(w_value.shape, BF16),
            vmem(w_out.shape, BF16),
            vmem((depth, units * rows, local_width), BF16),
            vmem((depth, units * rows, local_width), BF16),
            vmem((PIECES, tp, prows, width), F32),
            vmem((PIECES, tp, prows, width), BF16),
            vmem(results, BF16),
            vmem(results, BF16),
            vmem(results, BF16),
            vmem(notes, F32),
            vmem(notes, F32),
            vmem(results[:2] + (2,) + results[3:], BF16),
            vmem(notes[:2] + (2,) + notes[3:], F32),
            vmem((piece_rows, local_width), BF16),
            vmem((depth, PIECES, CORES, nx, prows, width), BF16),
            vmem((depth, PIECES, nx, prows, width), BF16),
            vmem((depth, PIECES, nx, CORES, nx, prows, width), BF16),
            vmem((2, PIECES, nx, prows, width), BF16),
            vmem((1024, 8, 128), F32),
            vmem(gains.shape, F32),
            dma((3,)), dma((3, depth)), dma((3,)), dma((nx,)),
            dma((units - 2, 4)), dma((1,)), dma((units - 2, 2)), dma((1,)), dma((depth - 1, PIECES, sp)),
            dma((nx - 1, 4 - SWAPPED)),
            dma((depth, PIECES)), dma((depth, PIECES, 2)), dma((depth, PIECES)),
            dma((depth - 1, PIECES, nx - 1)), dma((depth - 1, PIECES)), dma((PIECES, nx - 1)),
        ],
        compiler_params=pltpu.CompilerParams(
            collective_id=0, has_side_effects=True, vmem_limit_bytes=VMEM_KIB * 1024),
    )(*[pltpu.with_memory_space_constraint(one, pltpu.HBM) for one in (
        target, source, w_query, w_key, w_value, w_out, gains)])


def split_heads(row_block):
    return row_block.reshape(row_block.shape[0], row_block.shape[1] // HEAD, HEAD)


def body(target, source, w_query, w_key, w_value, w_out, gains):
    local_width = w_query.shape[2]
    score_scale = HEAD ** (-0.5)
    depth = w_query.shape[0]
    project_shard_part = lax.all_gather(source, "tp", axis=0, tiled=True)
    layer_parts = [
        jnp.stack(
            [
                jnp.dot(project_shard_part, w_key[level], preferred_element_type=jnp.float32),
                jnp.dot(project_shard_part, w_value[level], preferred_element_type=jnp.float32),
            ]
        )
        for level in range(depth)
    ]
    projected_source = jnp.stack(layer_parts).astype(jnp.bfloat16)
    stream = target.astype(jnp.float32)
    for layer_index in range(depth):
        normed = normalize(stream, gains[layer_index, 0]).astype(jnp.bfloat16)
        query_weight = w_query[layer_index]
        queries = jnp.dot(
            lax.all_gather(normed, "tp", axis=0, tiled=True),
            query_weight,
            preferred_element_type=jnp.float32,
        ).astype(jnp.bfloat16)
        row_count = queries.shape[0]
        keys_here = projected_source[layer_index, 0]
        values_here = projected_source[layer_index, 1]
        every_query = lax.all_gather(queries, "sp", axis=0, tiled=True)
        scores = (
            jnp.einsum(
                "qhd,khd->hqk",
                split_heads(every_query),
                split_heads(keys_here),
                preferred_element_type=jnp.float32,
            )
            * score_scale
        )
        row_peak = lax.pmax(jnp.max(scores, axis=2), "sp")
        weights = jnp.exp(scores - row_peak[:, :, None])
        local_summed = jnp.einsum(
            "hqk,khd->hqd",
            weights.astype(jnp.bfloat16),
            split_heads(values_here),
            preferred_element_type=jnp.float32,
        )
        summed, row_total = (
            lax.psum_scatter(
                local_summed.astype(jnp.bfloat16), "sp", scatter_dimension=1, tiled=True
            ).astype(jnp.float32),
            lax.psum_scatter(
                jnp.sum(weights, axis=2).astype(jnp.bfloat16), "sp", scatter_dimension=1, tiled=True
            ).astype(jnp.float32),
        )
        heads_out = summed / row_total[:, :, None]
        attended = (
            jnp.transpose(heads_out, (1, 0, 2)).reshape(row_count, local_width).astype(jnp.bfloat16)
        )
        out_weight = w_out[layer_index]
        projected = lax.psum_scatter(
            jnp.dot(attended, out_weight, preferred_element_type=jnp.float32).astype(jnp.bfloat16),
            "tp",
            scatter_dimension=0,
            tiled=True,
        ).astype(jnp.float32)
        stream = stream + normalize(projected, gains[layer_index, 1])
    return stream.astype(jnp.bfloat16)


def solution(mesh):
    in_specs = (
        P(("grp", "sp", "tp"), None),
        P(("grp", "sp", "tp"), None),
        P(None, None, "tp"),
        P(None, None, "tp"),
        P(None, None, "tp"),
        P(None, "tp", None),
        P(),
    )
    out_specs = P(("grp", "sp", "tp"), None)
    sp, tp = mesh.shape["sp"], mesh.shape["tp"]

    def run(target, source, w_query, w_key, w_value, w_out, gains):
        trows, rows, local_width = target.shape[0], source.shape[0], w_query.shape[2]
        tiles = (trows % (16 * PIECES) == 0 and tp * trows == PIECES * (HEAD // 2) and rows % 128 == 0
                 and sp % 2 == 0 and sp // 2 == 2 and w_query.shape[0] > 1 and tp > CORES
                 and local_width % (4 * HEAD) == 0 and tp % CORES == 0)
        form = functools.partial(fused_body, tp // CORES, sp) if tiles else body
        return form(target, source, w_query, w_key, w_value, w_out, gains)

    return jax.shard_map(run, mesh=mesh, in_specs=in_specs, out_specs=out_specs, check_vma=False)
```

```python
import functools
import math

import jax
import jax.numpy as jnp
from jax import lax
from jax.experimental import pallas as pl
from jax.experimental.pallas import tpu as pltpu
from jax.sharding import PartitionSpec as P

HEAD = 128
CORES = 2
PIECES = 2
SWAPPED = 2
VMEM_KIB = 54000


EPS = 1e-06
MESH = pl.DeviceIdType.MESH
F32 = jnp.float32
BF16 = jnp.bfloat16


def normalize(row_block, gain_row):
    return (
        row_block
        * lax.rsqrt(jnp.mean(row_block * row_block, axis=-1, keepdims=True) + EPS)
        * gain_row
    )


def fused_kernel(
    nx, sp, depth,
    target, source, w_query, w_key, w_value, w_out, gain_rows, out,
    tbuf, sbuf, wq, wk, wv, wo, keys, values, stream, normed, qbuf,
    osend, orecv, ssend, srecv, orelay, srelay, attended, pbuf, half_in, chip_sum, fin, ledger, gains,
    early_sum, early_peak, early_total,
    local_sem, weight_sem, send_sem, t_recv, s_recv, p_recv, r_recv, first_recv, q_recv,
    x_recv, o_recv, m_recv, h_recv, c_recv, d_recv, f_recv,
):
    s = lax.axis_index("sp")
    t = lax.axis_index("tp")
    x = t // CORES
    c = t % CORES
    partner_c = 1 - c
    partner = {"tp": x * CORES + partner_c}
    units = sbuf.shape[0]
    half = sbuf.shape[2]
    width = sbuf.shape[3]
    rows = 2 * half
    local_width = wk.shape[2]
    heads = local_width // HEAD
    tp = nx * CORES
    prows = stream.shape[2]
    piece_rows = tp * prows
    score_scale = HEAD ** (-0.5) * math.log2(math.e)

    pairs = sp // 2
    edge = jnp.logical_or(s == 0, s == sp - 1)
    inner = jnp.logical_not(edge)
    low = s < pairs
    near = jnp.where(s % 2 == 0, s + 1, s - 1)
    far_edge = jnp.where(low, sp - 1, 0)
    far_inner = jnp.where(low, pairs, pairs - 1)

    def chip(step):
        return lax.rem(x + step, nx)

    def peer(step):
        return {"tp": chip(step) * CORES + c}

    def remote(src, dst, send_sem, recv_sem, device):
        return pltpu.make_async_remote_copy(
            src_ref=src, dst_ref=dst, send_sem=send_sem, recv_sem=recv_sem,
            device_id=device, device_id_type=MESH,
        )

    def arrived(sem, *shapes):
        total = sum(math.prod(shape) * size for shape, size in shapes)
        block = ledger.at[pl.ds(0, total // math.prod(ledger.shape[1:]) // 4)]
        pltpu.make_async_copy(block, block, sem).wait()

    target_rows = (tbuf.shape[1:], 2)
    source_part = (sbuf.shape[2:], 2)
    result_block = (osend.shape[3:], 2)
    stats_block = (ssend.shape[3:], 4)
    sum_block = (half_in.shape[3:], 2)
    chip_rows = (half_in.shape[2:], 2)
    weight_block = (wk.shape[1:], 2)

    own_target = pltpu.make_async_copy(target, tbuf.at[t], local_sem.at[0])
    own_source = [
        pltpu.make_async_copy(
            source.at[pl.ds(part * half, half)], sbuf.at[0, part], local_sem.at[1])
        for part in range(2)
    ]

    def load(kind, level):
        pair = ((w_query, wq), (w_key, wk), (w_value, wv), (w_out, wo))[kind]
        return pltpu.make_async_copy(
            pair[0].at[level], pair[1].at[level], weight_sem.at[(0, 1, 1, 2)[kind], level])

    own_gains = pltpu.make_async_copy(gain_rows, gains, local_sem.at[2])
    own_target.start()
    own_gains.start()
    for copy in own_source:
        copy.start()
    load(1, 0).start()
    load(2, 0).start()

    barrier = pltpu.get_barrier_semaphore()
    pl.semaphore_signal(barrier, inc=1, device_id=partner, device_id_type=MESH)
    for step in range(1, nx):
        pl.semaphore_signal(barrier, inc=1, device_id=peer(step), device_id_type=MESH)
        pl.semaphore_signal(
            barrier, inc=1, device_id={"tp": chip(step) * CORES + partner_c}, device_id_type=MESH)
    for step in range(1, sp):
        pl.semaphore_signal(
            barrier, inc=1, device_id={"sp": lax.rem(s + step, sp)}, device_id_type=MESH)
    with jax.named_scope("barrier"):
        pl.semaphore_wait(barrier, 1 + 2 * (nx - 1) + (sp - 1))

    spans = ((0, half // 2), (half // 2, half // 4), (3 * half // 4, half // 8), (7 * half // 8, half // 8))
    swapped_rows = half - spans[SWAPPED][0]
    SOURCE, LINE, ROW = range(3)
    sent = {SOURCE: [], LINE: [], ROW: []}

    def go(copy, kind, shape):
        copy.start()
        sent[kind].append(shape)

    for step in range(1, nx):
        go(remote(target, tbuf.at[t], send_sem.at[SOURCE], t_recv.at[step], peer(step)),
           SOURCE, target_rows)
    go(remote(target, tbuf.at[t], send_sem.at[SOURCE], t_recv.at[0], partner), SOURCE, target_rows)
    for part in range(2):
        block = source.at[pl.ds(part * half, half)]
        for piece, (at, size) in enumerate(spans):
            span = pl.ds(at, size)
            for step in range(1, nx):
                unit = 2 * (nx - step) + part
                copy = remote(block.at[span], sbuf.at[unit, 0, span], send_sem.at[SOURCE],
                              s_recv.at[unit - 2, piece], peer(step))
                if part == 1 and piece >= SWAPPED:
                    pl.when(c == 1)(copy.start)
                    sent[SOURCE].append(((size, width), 2))

                    @pl.when(c == 0)
                    def _():
                        remote(block.at[span], sbuf.at[unit, 1, span], send_sem.at[SOURCE],
                               x_recv.at[nx - step - 1, piece - SWAPPED],
                               {"tp": chip(step) * CORES + 1}).start()
                else:
                    go(copy, SOURCE, ((size, width), 2))
        go(remote(block, sbuf.at[1, part], send_sem.at[SOURCE], p_recv.at[0], partner),
           SOURCE, source_part)

    def project(index):
        unit = index // depth
        level = index % depth
        with jax.named_scope("project"):
            block = sbuf[unit].reshape(rows, width)
            start = pl.multiple_of(unit * rows, rows)
            k = jnp.dot(block, wk[level], preferred_element_type=F32)
            keys[level, pl.ds(start, rows), :] = k.astype(BF16)
            v = jnp.dot(block, wv[level], preferred_element_type=F32)
            values[level, pl.ds(start, rows), :] = v.astype(BF16)

    def project_half(unit, level, part):
        with jax.named_scope("project_half"):
            block = sbuf[unit, :, pl.ds(part * (half // 2), half // 2)].reshape(half, width)
            start = pl.multiple_of(unit * rows + part * half, half)
            k = jnp.dot(block, wk[level], preferred_element_type=F32)
            keys[level, pl.ds(start, half), :] = k.astype(BF16)
            v = jnp.dot(block, wv[level], preferred_element_type=F32)
            values[level, pl.ds(start, half), :] = v.astype(BF16)

    def query_copy(level, p, block, j):
        sem = first_recv.at[0] if level == 0 else q_recv.at[level - 1, p, block]
        rows_of = qbuf.at[level, p, block]
        return remote(rows_of, rows_of, send_sem.at[LINE], sem, {"sp": j})

    def forward(level, p):
        @pl.when(inner)
        def _():
            for block in (far_inner, far_edge):
                arrived(q_recv.at[level - 1, p, block], result_block)
                query_copy(level, p, block, near).start()

    def hand_on(level, p):
        forward(level, p)

        @pl.when(jnp.logical_and(inner, p + 1 < PIECES))
        def _():
            query_copy(level, p + 1, s, near).start()

    def send_queries(level, p):
        if level == 0:
            query_copy(level, p, s, far_edge).start()
        query_copy(level, p, s, far_inner).start()
        if level == 0 or p == 0:
            query_copy(level, p, s, near).start()
        else:
            @pl.when(edge)
            def _():
                query_copy(level, p, s, near).start()

    def drain_line():
        def drain(queries):
            blocks = PIECES * ((depth + 1) * (sp - 1) + (depth - 1) * queries)
            arrived(send_sem.at[LINE], *([result_block] * blocks),
                    *([stats_block] * (depth * PIECES * (sp - 1))))

        @pl.when(edge)
        def _():
            drain(2)

        @pl.when(inner)
        def _():
            drain(4)

    def send_result(level, p, j):
        remote(osend.at[level, p, j], orecv.at[level, p, s], send_sem.at[LINE],
               o_recv.at[level, p], {"sp": j}).start()
        remote(ssend.at[level, p, j], srecv.at[level, p, s], send_sem.at[LINE],
               o_recv.at[level, p], {"sp": j}).start()

    def send_aside(level, p):
        for slot, j in enumerate((far_edge, far_inner)):
            remote(osend.at[level, p, j], orelay.at[level, p, slot], send_sem.at[LINE],
                   m_recv.at[level, p, slot], {"sp": near}).start()
            remote(ssend.at[level, p, j], srelay.at[level, p, slot], send_sem.at[LINE],
                   m_recv.at[level, p, slot], {"sp": near}).start()

    def source_relay(unit, piece):
        span = pl.ds(*spans[piece])
        return remote(sbuf.at[unit, 0, span], sbuf.at[unit, 1, span], send_sem.at[SOURCE],
                      r_recv.at[unit - 2, min(piece, 1)], partner)

    def relay_pieces(unit, pieces):
        for piece in pieces:
            arrived(s_recv.at[unit - 2, piece], ((spans[piece][1], width), 2))
            source_relay(unit, piece).start()

    def first_queries():
        own_target.wait()
        own_gains.wait()
        for step in range(1, nx):
            slot = chip(step) * CORES + c
            arrived(t_recv.at[step], target_rows)
            go(remote(tbuf.at[slot], tbuf.at[slot], send_sem.at[SOURCE], t_recv.at[0], partner),
               SOURCE, target_rows)
        arrived(t_recv.at[0], *([target_rows] * nx))

        @pl.loop(0, tp)
        def _(block):
            value = tbuf[block].astype(F32)
            ready = normalize(value, gains[0, 0:1, :]).astype(BF16)
            for p in range(PIECES):
                span = slice(p * prows, (p + 1) * prows)
                stream[p, block] = value[span]
                normed[p, block] = ready[span]

        load(0, 0).wait()
        q = jnp.dot(normed[...].reshape(PIECES * piece_rows, width), wq[0],
                    preferred_element_type=F32)
        for p in range(PIECES):
            qbuf[0, p, s] = q[p * piece_rows:(p + 1) * piece_rows].astype(BF16)
            send_queries(0, p)

    own_pair = s // 2
    every = slice(0, units * rows)
    early = slice(0, (units - 1) * rows)
    late = slice((units - 1) * rows, units * rows)

    def head_scores(layer, q, h, span):
        cols = slice(h * HEAD, (h + 1) * HEAD)
        scores = lax.dot_general(
            q[:, cols], keys[layer, span, cols], (((1,), (1,)), ((), ())), preferred_element_type=F32)
        return scores, jnp.max(scores, axis=1, keepdims=True) * score_scale

    def attend_early(p):
        with jax.named_scope("attend_early"):
            count = 2 * piece_rows
            q = qbuf[0, p, pl.ds(2 * (1 - own_pair), 2)].reshape(count, local_width)
            ahead = head_scores(0, q, 0, early)
            for h in range(heads):
                scores, peak = ahead
                if h + 1 < heads:
                    ahead = head_scores(0, q, h + 1, early)
                cols = slice(h * HEAD, (h + 1) * HEAD)
                weights = jnp.exp2(scores * score_scale - peak)
                total = jnp.sum(weights, axis=1, keepdims=True)
                early_sum[p, :, cols] = jnp.dot(
                    weights.astype(BF16), values[0, early, cols], preferred_element_type=F32)
                early_peak[p, :, cols] = jnp.broadcast_to(peak, (count, HEAD))
                early_total[p, :, cols] = jnp.broadcast_to(total, (count, HEAD))

    @pl.loop(0, units * depth - (depth - 1))
    def _(index):
        unit = index // depth
        level = index % depth

        @pl.when(index == 0)
        def _():
            arrived(local_sem.at[1], source_part, source_part)
            arrived(weight_sem.at[1, 0], weight_block, weight_block)
            load(0, 0).start()
            for later in range(1, depth):
                load(1, later).start()
                load(2, later).start()
            load(3, 0).start()
            for later in range(1, depth):
                load(0, later).start()
                load(3, later).start()

        for later in range(1, depth):
            @pl.when(index == later)
            def _():
                arrived(weight_sem.at[1, later], weight_block, weight_block)

        @pl.when(index == depth)
        def _():
            with jax.named_scope("first_queries"):
                first_queries()
            arrived(p_recv.at[0], source_part, source_part)

        @pl.when(index == (units - 1) * depth)
        def _():
            arrived(first_recv.at[0], *([result_block] * (PIECES * (sp - 1))))

            @pl.loop(0, PIECES)
            def _(p):
                attend_early(p)

        @pl.when(jnp.logical_and(unit >= 2, level == 0))
        def _():
            with jax.named_scope("wait_remote"):
                relay_pieces(unit, (0,))
                arrived(r_recv.at[unit - 2, 0], ((half // 2, width), 2))

            @pl.when(unit == units - 1)
            def _():
                project_half(unit, level, 0)

            with jax.named_scope("wait_remote2"):
                relay_pieces(unit, range(1, SWAPPED))
                shared = unit % 2 == 1

                @pl.when(jnp.logical_or(c == 1, jnp.logical_not(shared)))
                def _():
                    relay_pieces(unit, range(SWAPPED, len(spans)))

                @pl.when(jnp.logical_and(c == 1, shared))
                def _():
                    for piece in range(SWAPPED, len(spans)):
                        span = pl.ds(*spans[piece])
                        arrived(x_recv.at[(unit - 3) // 2, piece - SWAPPED], ((spans[piece][1], width), 2))
                        remote(sbuf.at[unit, 1, span], sbuf.at[unit, 0, span], send_sem.at[SOURCE],
                               r_recv.at[unit - 2, 1], partner).start()

            with jax.named_scope("wait_relayed"):
                @pl.when(jnp.logical_not(shared))
                def _():
                    arrived(r_recv.at[unit - 2, 1], ((half // 2, width), 2))

                @pl.when(jnp.logical_and(c == 0, shared))
                def _():
                    arrived(r_recv.at[unit - 2, 1], ((half // 2 + swapped_rows, width), 2))

                @pl.when(jnp.logical_and(c == 1, shared))
                def _():
                    arrived(r_recv.at[unit - 2, 1], ((half // 2 - swapped_rows, width), 2))

            @pl.when(unit == units - 1)
            def _():
                project_half(unit, level, 1)

        @pl.when(index < (units - 1) * depth)
        def _():
            project(index)

    sent[SOURCE] += [source_part] * (units - 2 - (nx - 1))
    sent[SOURCE] += [((half - swapped_rows, width), 2)] * (nx - 1)

    def columns(parts):
        stacked = jnp.concatenate(parts, axis=0)
        fill = jnp.zeros((HEAD - stacked.shape[0], stacked.shape[1]), F32)
        return jnp.concatenate([stacked, fill], axis=0).T

    def weighted(cols, blocks, h):
        span = slice(h * HEAD, (h + 1) * HEAD)
        return sum(
            cols[0:piece_rows, k * heads + h:k * heads + h + 1] * block[:, span].astype(F32)
            for k, block in enumerate(blocks))

    def merge(layer, p):
        @pl.when(inner)
        def _():
            for slot, j in enumerate((far_edge, far_inner)):
                with jax.named_scope("merge_wait"):
                    arrived(m_recv.at[layer, p, slot], result_block, stats_block)
                with jax.named_scope("merge"):
                    mine, theirs = ssend[layer, p, j], srelay[layer, p, slot]
                    top = jnp.maximum(mine[0:heads], theirs[0:heads])
                    share = [jnp.exp2(one[0:heads] - top) for one in (mine, theirs)]
                    total = share[0] * mine[heads:] + share[1] * theirs[heads:]
                    cols = columns(share)
                    blocks = (osend[layer, p, j], orelay[layer, p, slot])
                    for h in range(heads):
                        osend[layer, p, j, :, h * HEAD:(h + 1) * HEAD] = weighted(
                            cols, blocks, h).astype(BF16)
                    ssend[layer, p, j] = jnp.concatenate([top, total], axis=0)
                    send_result(layer, p, j)

    def attend(layer, p, first, blocks, span, started=False):
        with jax.named_scope("attend"):
            count = blocks * piece_rows
            q = qbuf[layer, p, pl.ds(first, blocks)].reshape(count, local_width)
            lane = lax.broadcasted_iota(jnp.int32, (count, HEAD), 1)
            notes = jnp.zeros((count, HEAD), F32)
            ahead = head_scores(layer, q, 0, span)
            for h in range(heads):
                scores, peak = ahead
                if h + 1 < heads:
                    ahead = head_scores(layer, q, h + 1, span)
                cols = slice(h * HEAD, (h + 1) * HEAD)
                if started:
                    before = early_peak[p, :, cols]
                    peak = jnp.maximum(before, peak)
                    fade = jnp.exp2(before - peak)
                    shift = jnp.concatenate(
                        [peak] * (scores.shape[1] // HEAD), axis=1)
                    weights = jnp.exp2(scores * score_scale - shift)
                    total = jnp.sum(weights, axis=1, keepdims=True) + fade * early_total[p, :, cols]
                    o = jnp.dot(weights.astype(BF16), values[layer, span, cols], preferred_element_type=F32)
                    o = o + fade * early_sum[p, :, cols]
                else:
                    weights = jnp.exp2(scores * score_scale - peak)
                    total = jnp.sum(weights, axis=1, keepdims=True)
                    o = jnp.dot(weights.astype(BF16), values[layer, span, cols], preferred_element_type=F32)
                o = o.astype(BF16)
                for member in range(blocks):
                    osend[layer, p, first + member, :, cols] = o[member * piece_rows:(member + 1) * piece_rows]
                notes = jnp.where(lane == h, peak, notes)
                notes = jnp.where(lane == heads + h, total, notes)
            for two in range(blocks // 2):
                stats = notes[two * HEAD:(two + 1) * HEAD].T[0:2 * heads]
                ssend[layer, p, first + 2 * two] = stats
                ssend[layer, p, first + 2 * two + 1] = pltpu.roll(stats, piece_rows, 1)

    def keep_own(layer, p):
        orecv[layer, p, s] = osend[layer, p, s]
        srecv[layer, p, s] = ssend[layer, p, s]

    def out_project(layer, p):
        with jax.named_scope("wait_o"):
            arrived(o_recv.at[layer, p], *([result_block, stats_block] * 2))
        with jax.named_scope("combine_out"):
            origins = (s, near, far_inner)
            stats = [srecv[layer, p, j] for j in origins]
            top = functools.reduce(jnp.maximum, [one[0:heads] for one in stats])
            share = [jnp.exp2(one[0:heads] - top) for one in stats]
            total = sum(part * one[heads:] for part, one in zip(share, stats))
            cols = columns([part / total for part in share])
            blocks = [orecv[layer, p, j] for j in origins]
            for h in range(heads):
                attended[:, h * HEAD:(h + 1) * HEAD] = weighted(cols, blocks, h).astype(BF16)
            tile = min(512, width)
            for n in range(width // tile):
                span = slice(n * tile, (n + 1) * tile)
                part = jnp.dot(attended[...], wo[layer, :, span], preferred_element_type=F32).astype(BF16)
                for b in range(nx):
                    for core in range(CORES):
                        at = (b * CORES + core) * prows
                        pbuf[layer, p, core, b, :, span] = part[at:at + prows]
            go(remote(pbuf.at[layer, p, partner_c], half_in.at[layer, p], send_sem.at[ROW],
                      h_recv.at[layer, p], partner), ROW, chip_rows)

    def chip_total(layer, p):
        with jax.named_scope("chip_total"):
            arrived(h_recv.at[layer, p], chip_rows)
            for b in range(nx):
                both_cores = pbuf[layer, p, c, b].astype(F32) + half_in[layer, p, b].astype(F32)
                chip_sum[layer, p, x, c, b] = both_cores.astype(BF16)
            own = chip_sum.at[layer, p, x, c]
            for step in range(1, nx):
                go(remote(own, own, send_sem.at[ROW], c_recv.at[layer, p, nx - step - 1], peer(step)),
                   ROW, chip_rows)
            go(remote(own, own, send_sem.at[ROW], d_recv.at[layer, p], partner), ROW, chip_rows)

    def next_queries(layer, p):
        with jax.named_scope("xwait"):
            for step in range(1, nx):
                a = chip(step)
                other = chip_sum.at[layer, p, a, c]
                arrived(c_recv.at[layer, p, step - 1], chip_rows)
                go(remote(other, other, send_sem.at[ROW], d_recv.at[layer, p], partner), ROW, chip_rows)
            arrived(d_recv.at[layer, p], *([chip_rows] * nx))
        with jax.named_scope("norm_q"):
            for block in range(tp):
                projected = sum(
                    chip_sum[layer, p, a, block % CORES, block // CORES].astype(F32) for a in range(nx))
                value = stream[p, block] + normalize(projected, gains[layer, 1:2, :])
                stream[p, block] = value
                normed[p, block] = normalize(value, gains[layer + 1, 0:1, :]).astype(BF16)
            q = jnp.dot(normed[p].reshape(piece_rows, width), wq[layer + 1],
                        preferred_element_type=F32)
            qbuf[layer + 1, p, s] = q.astype(BF16)
            send_queries(layer + 1, p)

    def final_send(layer, p):
        with jax.named_scope("final_send"):
            arrived(h_recv.at[layer, p], chip_rows)
            for step in range(1, nx):
                b = chip(step)
                both_cores = pbuf[layer, p, c, b].astype(F32) + half_in[layer, p, b].astype(F32)
                fin[0, p, b] = both_cores.astype(BF16)
                go(remote(fin.at[0, p, b], fin.at[1, p, x], send_sem.at[ROW],
                          f_recv.at[p, nx - step - 1], peer(step)), ROW, sum_block)

    def final_rows(layer, p):
        with jax.named_scope("final_rows"):
            projected = pbuf[layer, p, c, x].astype(F32) + half_in[layer, p, x].astype(F32)
            for step in range(1, nx):
                b = chip(step)
                arrived(f_recv.at[p, step - 1], sum_block)
                projected = projected + fin[1, p, b].astype(F32)
            value = stream[p, t] + normalize(projected, gains[layer, 1:2, :])
            out[p * prows:(p + 1) * prows, :] = value.astype(out.dtype)

    for layer in range(depth):
        last = layer == depth - 1
        if layer > 0:
            hand_on(layer, 0)
        if layer == 1:
            @pl.loop(units * depth - (depth - 1), units * depth)
            def _(index):
                project(index)

        if layer == 0:
            @pl.loop(0, PIECES)
            def _(p):
                attend(layer, p, 2 * (1 - own_pair), 2, late, started=True)

                @pl.when(edge)
                def _():
                    send_aside(layer, p)

            @pl.loop(0, PIECES)
            def _(p):
                attend(layer, p, 2 * own_pair, 2, every)
                send_result(layer, p, near)
                keep_own(layer, p)
        else:
            @pl.loop(0, 2 * PIECES)
            def _(i):
                p, close = i // 2, i % 2 == 0

                @pl.when(close)
                def _():
                    @pl.when(p > 0)
                    def _():
                        hand_on(layer, p)

                    with jax.named_scope("wait_near"):
                        arrived(q_recv.at[layer - 1, p, near], result_block)

                @pl.when(jnp.logical_and(edge, jnp.logical_not(close)))
                def _():
                    with jax.named_scope("wait_far"):
                        for block in (far_inner, far_edge):
                            arrived(q_recv.at[layer - 1, p, block], result_block)

                attend(layer, p, jnp.where(close, 2 * own_pair, 2 * (1 - own_pair)), 2, every)

                @pl.when(close)
                def _():
                    keep_own(layer, p)

                @pl.when(jnp.logical_and(edge, close))
                def _():
                    send_result(layer, p, near)

                @pl.when(jnp.logical_and(inner, i == 2 * PIECES - 2))
                def _():
                    for later in range(PIECES):
                        send_result(layer, later, near)

                @pl.when(jnp.logical_and(edge, jnp.logical_not(close)))
                def _():
                    send_aside(layer, p)

        total = final_send if last else chip_total
        load(3, layer).wait()
        for p in range(PIECES):
            merge(layer, p)
        for p in range(PIECES):
            out_project(layer, p)
            total(layer, p)
        if not last:
            load(0, layer + 1).wait()
        for p in range(PIECES):
            if last:
                final_rows(layer, p)
            else:
                next_queries(layer, p)

    with jax.named_scope("finish"):
        drain_line()
        arrived(send_sem.at[ROW], *sent[ROW])
        moved = ((swapped_rows * (nx - 1), width), 2)

        @pl.when(c == 0)
        def _():
            arrived(send_sem.at[SOURCE], *sent[SOURCE])

        @pl.when(c == 1)
        def _():
            arrived(send_sem.at[SOURCE], *sent[SOURCE], moved, moved)


def fused_body(nx, sp, target, source, w_query, w_key, w_value, w_out, gains):
    depth, width, local_width = w_query.shape
    trows, rows = target.shape[0], source.shape[0]
    tp = nx * CORES
    prows = trows // PIECES
    piece_rows = tp * prows
    heads = local_width // HEAD
    units = 2 * nx
    vmem = pltpu.VMEM
    dma = pltpu.SemaphoreType.DMA
    anywhere = pl.BlockSpec(memory_space=pl.ANY)
    whole = pl.BlockSpec(memory_space=pltpu.VMEM)
    results = (depth, PIECES, sp, piece_rows, local_width)
    notes = (depth, PIECES, sp, 2 * heads, 2 * piece_rows)
    return pl.pallas_call(
        functools.partial(fused_kernel, nx, sp, depth),
        out_shape=jax.ShapeDtypeStruct((trows, width), BF16),
        in_specs=[anywhere] * 7,
        out_specs=whole,
        scratch_shapes=[
            vmem((tp, trows, width), BF16),
            vmem((units, 2, rows // 2, width), BF16),
            vmem(w_query.shape, BF16),
            vmem(w_key.shape, BF16),
            vmem(w_value.shape, BF16),
            vmem(w_out.shape, BF16),
            vmem((depth, units * rows, local_width), BF16),
            vmem((depth, units * rows, local_width), BF16),
            vmem((PIECES, tp, prows, width), F32),
            vmem((PIECES, tp, prows, width), BF16),
            vmem(results, BF16),
            vmem(results, BF16),
            vmem(results, BF16),
            vmem(notes, F32),
            vmem(notes, F32),
            vmem(results[:2] + (2,) + results[3:], BF16),
            vmem(notes[:2] + (2,) + notes[3:], F32),
            vmem((piece_rows, local_width), BF16),
            vmem((depth, PIECES, CORES, nx, prows, width), BF16),
            vmem((depth, PIECES, nx, prows, width), BF16),
            vmem((depth, PIECES, nx, CORES, nx, prows, width), BF16),
            vmem((2, PIECES, nx, prows, width), BF16),
            vmem((1024, 8, 128), F32),
            vmem(gains.shape, F32),
            vmem((PIECES, 2 * piece_rows, local_width), F32),
            vmem((PIECES, 2 * piece_rows, local_width), F32),
            vmem((PIECES, 2 * piece_rows, local_width), F32),
            dma((3,)), dma((3, depth)), dma((3,)), dma((nx,)),
            dma((units - 2, 4)), dma((1,)), dma((units - 2, 2)), dma((1,)), dma((depth - 1, PIECES, sp)),
            dma((nx - 1, 4 - SWAPPED)),
            dma((depth, PIECES)), dma((depth, PIECES, 2)), dma((depth, PIECES)),
            dma((depth - 1, PIECES, nx - 1)), dma((depth - 1, PIECES)), dma((PIECES, nx - 1)),
        ],
        compiler_params=pltpu.CompilerParams(
            collective_id=0, has_side_effects=True, vmem_limit_bytes=VMEM_KIB * 1024),
    )(*[pltpu.with_memory_space_constraint(one, pltpu.HBM) for one in (
        target, source, w_query, w_key, w_value, w_out, gains)])


def split_heads(row_block):
    return row_block.reshape(row_block.shape[0], row_block.shape[1] // HEAD, HEAD)


def body(target, source, w_query, w_key, w_value, w_out, gains):
    local_width = w_query.shape[2]
    score_scale = HEAD ** (-0.5)
    depth = w_query.shape[0]
    project_shard_part = lax.all_gather(source, "tp", axis=0, tiled=True)
    layer_parts = [
        jnp.stack(
            [
                jnp.dot(project_shard_part, w_key[level], preferred_element_type=jnp.float32),
                jnp.dot(project_shard_part, w_value[level], preferred_element_type=jnp.float32),
            ]
        )
        for level in range(depth)
    ]
    projected_source = jnp.stack(layer_parts).astype(jnp.bfloat16)
    stream = target.astype(jnp.float32)
    for layer_index in range(depth):
        normed = normalize(stream, gains[layer_index, 0]).astype(jnp.bfloat16)
        query_weight = w_query[layer_index]
        queries = jnp.dot(
            lax.all_gather(normed, "tp", axis=0, tiled=True),
            query_weight,
            preferred_element_type=jnp.float32,
        ).astype(jnp.bfloat16)
        row_count = queries.shape[0]
        keys_here = projected_source[layer_index, 0]
        values_here = projected_source[layer_index, 1]
        every_query = lax.all_gather(queries, "sp", axis=0, tiled=True)
        scores = (
            jnp.einsum(
                "qhd,khd->hqk",
                split_heads(every_query),
                split_heads(keys_here),
                preferred_element_type=jnp.float32,
            )
            * score_scale
        )
        row_peak = lax.pmax(jnp.max(scores, axis=2), "sp")
        weights = jnp.exp(scores - row_peak[:, :, None])
        local_summed = jnp.einsum(
            "hqk,khd->hqd",
            weights.astype(jnp.bfloat16),
            split_heads(values_here),
            preferred_element_type=jnp.float32,
        )
        summed, row_total = (
            lax.psum_scatter(
                local_summed.astype(jnp.bfloat16), "sp", scatter_dimension=1, tiled=True
            ).astype(jnp.float32),
            lax.psum_scatter(
                jnp.sum(weights, axis=2).astype(jnp.bfloat16), "sp", scatter_dimension=1, tiled=True
            ).astype(jnp.float32),
        )
        heads_out = summed / row_total[:, :, None]
        attended = (
            jnp.transpose(heads_out, (1, 0, 2)).reshape(row_count, local_width).astype(jnp.bfloat16)
        )
        out_weight = w_out[layer_index]
        projected = lax.psum_scatter(
            jnp.dot(attended, out_weight, preferred_element_type=jnp.float32).astype(jnp.bfloat16),
            "tp",
            scatter_dimension=0,
            tiled=True,
        ).astype(jnp.float32)
        stream = stream + normalize(projected, gains[layer_index, 1])
    return stream.astype(jnp.bfloat16)


def solution(mesh):
    in_specs = (
        P(("grp", "sp", "tp"), None),
        P(("grp", "sp", "tp"), None),
        P(None, None, "tp"),
        P(None, None, "tp"),
        P(None, None, "tp"),
        P(None, "tp", None),
        P(),
    )
    out_specs = P(("grp", "sp", "tp"), None)
    sp, tp = mesh.shape["sp"], mesh.shape["tp"]

    def run(target, source, w_query, w_key, w_value, w_out, gains):
        trows, rows, local_width = target.shape[0], source.shape[0], w_query.shape[2]
        tiles = (trows % (16 * PIECES) == 0 and tp * trows == PIECES * (HEAD // 2) and rows % 128 == 0
                 and sp % 2 == 0 and sp // 2 == 2 and w_query.shape[0] > 1 and tp > CORES
                 and local_width % (4 * HEAD) == 0 and tp % CORES == 0)
        form = functools.partial(fused_body, tp // CORES, sp) if tiles else body
        return form(target, source, w_query, w_key, w_value, w_out, gains)

    return jax.shard_map(run, mesh=mesh, in_specs=in_specs, out_specs=out_specs, check_vma=False)
```

```python
import functools
import math

import jax
import jax.numpy as jnp
from jax import lax
from jax.experimental import pallas as pl
from jax.experimental.pallas import tpu as pltpu
from jax.sharding import PartitionSpec as P

HEAD = 128
CORES = 2
PIECES = 2
SWAPPED = 2
VMEM_KIB = 54000


EPS = 1e-06
MESH = pl.DeviceIdType.MESH
F32 = jnp.float32
BF16 = jnp.bfloat16


def normalize(row_block, gain_row):
    return (
        row_block
        * lax.rsqrt(jnp.mean(row_block * row_block, axis=-1, keepdims=True) + EPS)
        * gain_row
    )


def fused_kernel(
    nx, sp, depth,
    target, source, w_query, w_key, w_value, w_out, gain_rows, out,
    tbuf, sbuf, wq, wk, wv, wo, keys, values, stream, normed, qbuf,
    osend, orecv, ssend, srecv, orelay, srelay, attended, pbuf, half_in, chip_sum, fin, ledger, gains,
    early_sum, early_peak, early_total,
    local_sem, weight_sem, send_sem, t_recv, s_recv, p_recv, r_recv, first_recv, q_recv,
    x_recv, o_recv, m_recv, h_recv, c_recv, d_recv, f_recv,
):
    s = lax.axis_index("sp")
    t = lax.axis_index("tp")
    x = t // CORES
    c = t % CORES
    partner_c = 1 - c
    partner = {"tp": x * CORES + partner_c}
    units = sbuf.shape[0]
    half = sbuf.shape[2]
    width = sbuf.shape[3]
    rows = 2 * half
    local_width = wk.shape[2]
    heads = local_width // HEAD
    tp = nx * CORES
    prows = stream.shape[2]
    piece_rows = tp * prows
    score_scale = HEAD ** (-0.5) * math.log2(math.e)

    pairs = sp // 2
    edge = jnp.logical_or(s == 0, s == sp - 1)
    inner = jnp.logical_not(edge)
    low = s < pairs
    near = jnp.where(s % 2 == 0, s + 1, s - 1)
    far_edge = jnp.where(low, sp - 1, 0)
    far_inner = jnp.where(low, pairs, pairs - 1)

    def chip(step):
        return lax.rem(x + step, nx)

    def peer(step):
        return {"tp": chip(step) * CORES + c}

    def remote(src, dst, send_sem, recv_sem, device):
        return pltpu.make_async_remote_copy(
            src_ref=src, dst_ref=dst, send_sem=send_sem, recv_sem=recv_sem,
            device_id=device, device_id_type=MESH,
        )

    def arrived(sem, *shapes):
        total = sum(math.prod(shape) * size for shape, size in shapes)
        block = ledger.at[pl.ds(0, total // math.prod(ledger.shape[1:]) // 4)]
        pltpu.make_async_copy(block, block, sem).wait()

    target_rows = (tbuf.shape[1:], 2)
    source_part = (sbuf.shape[2:], 2)
    result_block = (osend.shape[3:], 2)
    stats_block = (ssend.shape[3:], 4)
    sum_block = (half_in.shape[3:], 2)
    chip_rows = (half_in.shape[2:], 2)
    weight_block = (wk.shape[1:], 2)

    own_target = pltpu.make_async_copy(target, tbuf.at[t], local_sem.at[0])
    own_source = [
        pltpu.make_async_copy(
            source.at[pl.ds(part * half, half)], sbuf.at[0, part], local_sem.at[1])
        for part in range(2)
    ]

    def load(kind, level):
        pair = ((w_query, wq), (w_key, wk), (w_value, wv), (w_out, wo))[kind]
        return pltpu.make_async_copy(
            pair[0].at[level], pair[1].at[level], weight_sem.at[(0, 1, 1, 2)[kind], level])

    own_gains = pltpu.make_async_copy(gain_rows, gains, local_sem.at[2])
    own_target.start()
    own_gains.start()
    for copy in own_source:
        copy.start()
    load(1, 0).start()
    load(2, 0).start()

    barrier = pltpu.get_barrier_semaphore()
    pl.semaphore_signal(barrier, inc=1, device_id=partner, device_id_type=MESH)
    for step in range(1, nx):
        pl.semaphore_signal(barrier, inc=1, device_id=peer(step), device_id_type=MESH)
        pl.semaphore_signal(
            barrier, inc=1, device_id={"tp": chip(step) * CORES + partner_c}, device_id_type=MESH)
    for step in range(1, sp):
        pl.semaphore_signal(
            barrier, inc=1, device_id={"sp": lax.rem(s + step, sp)}, device_id_type=MESH)
    with jax.named_scope("barrier"):
        pl.semaphore_wait(barrier, 1 + 2 * (nx - 1) + (sp - 1))

    spans = ((0, half // 2), (half // 2, half // 4), (3 * half // 4, half // 8), (7 * half // 8, half // 8))
    swapped_rows = half - spans[SWAPPED][0]
    SOURCE, LINE, ROW = range(3)
    sent = {SOURCE: [], LINE: [], ROW: []}

    def go(copy, kind, shape):
        copy.start()
        sent[kind].append(shape)

    for step in range(1, nx):
        go(remote(target, tbuf.at[t], send_sem.at[SOURCE], t_recv.at[step], peer(step)),
           SOURCE, target_rows)
    go(remote(target, tbuf.at[t], send_sem.at[SOURCE], t_recv.at[0], partner), SOURCE, target_rows)
    for part in range(2):
        block = source.at[pl.ds(part * half, half)]
        for piece, (at, size) in enumerate(spans):
            span = pl.ds(at, size)
            for step in range(1, nx):
                unit = 2 * (nx - step) + part
                copy = remote(block.at[span], sbuf.at[unit, 0, span], send_sem.at[SOURCE],
                              s_recv.at[unit - 2, piece], peer(step))
                if part == 1 and piece >= SWAPPED:
                    pl.when(c == 1)(copy.start)
                    sent[SOURCE].append(((size, width), 2))

                    @pl.when(c == 0)
                    def _():
                        remote(block.at[span], sbuf.at[unit, 1, span], send_sem.at[SOURCE],
                               x_recv.at[nx - step - 1, piece - SWAPPED],
                               {"tp": chip(step) * CORES + 1}).start()
                else:
                    go(copy, SOURCE, ((size, width), 2))
        go(remote(block, sbuf.at[1, part], send_sem.at[SOURCE], p_recv.at[0], partner),
           SOURCE, source_part)

    def project(index):
        unit = index // depth
        level = index % depth
        with jax.named_scope("project"):
            block = sbuf[unit].reshape(rows, width)
            start = pl.multiple_of(unit * rows, rows)
            k = jnp.dot(block, wk[level], preferred_element_type=F32)
            keys[level, pl.ds(start, rows), :] = k.astype(BF16)
            v = jnp.dot(block, wv[level], preferred_element_type=F32)
            values[level, pl.ds(start, rows), :] = v.astype(BF16)

    def project_half(unit, level, part):
        with jax.named_scope("project_half"):
            block = sbuf[unit, :, pl.ds(part * (half // 2), half // 2)].reshape(half, width)
            start = pl.multiple_of(unit * rows + part * half, half)
            k = jnp.dot(block, wk[level], preferred_element_type=F32)
            keys[level, pl.ds(start, half), :] = k.astype(BF16)
            v = jnp.dot(block, wv[level], preferred_element_type=F32)
            values[level, pl.ds(start, half), :] = v.astype(BF16)

    def query_copy(level, p, block, j):
        sem = first_recv.at[0] if level == 0 else q_recv.at[level - 1, p, block]
        rows_of = qbuf.at[level, p, block]
        return remote(rows_of, rows_of, send_sem.at[LINE], sem, {"sp": j})

    def forward(level, p):
        @pl.when(inner)
        def _():
            for block in (far_inner, far_edge):
                arrived(q_recv.at[level - 1, p, block], result_block)
                query_copy(level, p, block, near).start()

    def hand_on(level, p):
        forward(level, p)

        @pl.when(jnp.logical_and(inner, p == PIECES - 1))
        def _():
            for held in range(1, PIECES):
                query_copy(level, held, s, near).start()

    def send_queries(level, p):
        if level == 0:
            query_copy(level, p, s, far_edge).start()
        query_copy(level, p, s, far_inner).start()
        if level == 0 or p == 0:
            query_copy(level, p, s, near).start()
        else:
            @pl.when(edge)
            def _():
                query_copy(level, p, s, near).start()

    def drain_line():
        def drain(queries):
            blocks = PIECES * ((depth + 1) * (sp - 1) + (depth - 1) * queries)
            arrived(send_sem.at[LINE], *([result_block] * blocks),
                    *([stats_block] * (depth * PIECES * (sp - 1))))

        @pl.when(edge)
        def _():
            drain(2)

        @pl.when(inner)
        def _():
            drain(4)

    def send_result(level, p, j):
        remote(osend.at[level, p, j], orecv.at[level, p, s], send_sem.at[LINE],
               o_recv.at[level, p], {"sp": j}).start()
        remote(ssend.at[level, p, j], srecv.at[level, p, s], send_sem.at[LINE],
               o_recv.at[level, p], {"sp": j}).start()

    def send_aside(level, p):
        for slot, j in enumerate((far_edge, far_inner)):
            remote(osend.at[level, p, j], orelay.at[level, p, slot], send_sem.at[LINE],
                   m_recv.at[level, p, slot], {"sp": near}).start()
            remote(ssend.at[level, p, j], srelay.at[level, p, slot], send_sem.at[LINE],
                   m_recv.at[level, p, slot], {"sp": near}).start()

    def source_relay(unit, piece):
        span = pl.ds(*spans[piece])
        return remote(sbuf.at[unit, 0, span], sbuf.at[unit, 1, span], send_sem.at[SOURCE],
                      r_recv.at[unit - 2, min(piece, 1)], partner)

    def relay_pieces(unit, pieces):
        for piece in pieces:
            arrived(s_recv.at[unit - 2, piece], ((spans[piece][1], width), 2))
            source_relay(unit, piece).start()

    def first_queries():
        own_target.wait()
        own_gains.wait()
        for step in range(1, nx):
            slot = chip(step) * CORES + c
            arrived(t_recv.at[step], target_rows)
            go(remote(tbuf.at[slot], tbuf.at[slot], send_sem.at[SOURCE], t_recv.at[0], partner),
               SOURCE, target_rows)
        arrived(t_recv.at[0], *([target_rows] * nx))

        @pl.loop(0, tp)
        def _(block):
            value = tbuf[block].astype(F32)
            ready = normalize(value, gains[0, 0:1, :]).astype(BF16)
            for p in range(PIECES):
                span = slice(p * prows, (p + 1) * prows)
                stream[p, block] = value[span]
                normed[p, block] = ready[span]

        load(0, 0).wait()
        q = jnp.dot(normed[...].reshape(PIECES * piece_rows, width), wq[0],
                    preferred_element_type=F32)
        for p in range(PIECES):
            qbuf[0, p, s] = q[p * piece_rows:(p + 1) * piece_rows].astype(BF16)
            send_queries(0, p)

    own_pair = s // 2
    every = slice(0, units * rows)
    early = slice(0, (units - 1) * rows)
    late = slice((units - 1) * rows, units * rows)

    def head_scores(layer, q, h, span):
        cols = slice(h * HEAD, (h + 1) * HEAD)
        scores = lax.dot_general(
            q[:, cols], keys[layer, span, cols], (((1,), (1,)), ((), ())), preferred_element_type=F32)
        return scores, jnp.max(scores, axis=1, keepdims=True) * score_scale

    def attend_early(p):
        with jax.named_scope("attend_early"):
            count = 2 * piece_rows
            q = qbuf[0, p, pl.ds(2 * (1 - own_pair), 2)].reshape(count, local_width)
            ahead = head_scores(0, q, 0, early)
            for h in range(heads):
                scores, peak = ahead
                if h + 1 < heads:
                    ahead = head_scores(0, q, h + 1, early)
                cols = slice(h * HEAD, (h + 1) * HEAD)
                weights = jnp.exp2(scores * score_scale - peak)
                total = jnp.sum(weights, axis=1, keepdims=True)
                early_sum[p, :, cols] = jnp.dot(
                    weights.astype(BF16), values[0, early, cols], preferred_element_type=F32)
                early_peak[p, :, cols] = jnp.broadcast_to(peak, (count, HEAD))
                early_total[p, :, cols] = jnp.broadcast_to(total, (count, HEAD))

    @pl.loop(0, units * depth - (depth - 1))
    def _(index):
        unit = index // depth
        level = index % depth

        @pl.when(index == 0)
        def _():
            arrived(local_sem.at[1], source_part, source_part)
            arrived(weight_sem.at[1, 0], weight_block, weight_block)
            load(0, 0).start()
            for later in range(1, depth):
                load(1, later).start()
                load(2, later).start()
            load(3, 0).start()
            for later in range(1, depth):
                load(0, later).start()
                load(3, later).start()

        for later in range(1, depth):
            @pl.when(index == later)
            def _():
                arrived(weight_sem.at[1, later], weight_block, weight_block)

        @pl.when(index == depth)
        def _():
            with jax.named_scope("first_queries"):
                first_queries()
            arrived(p_recv.at[0], source_part, source_part)

        @pl.when(index == (units - 1) * depth)
        def _():
            arrived(first_recv.at[0], *([result_block] * (PIECES * (sp - 1))))

            @pl.loop(0, PIECES)
            def _(p):
                attend_early(p)

        @pl.when(jnp.logical_and(unit >= 2, level == 0))
        def _():
            with jax.named_scope("wait_remote"):
                relay_pieces(unit, (0,))
                arrived(r_recv.at[unit - 2, 0], ((half // 2, width), 2))

            @pl.when(unit == units - 1)
            def _():
                project_half(unit, level, 0)

            with jax.named_scope("wait_remote2"):
                relay_pieces(unit, range(1, SWAPPED))
                shared = unit % 2 == 1

                @pl.when(jnp.logical_or(c == 1, jnp.logical_not(shared)))
                def _():
                    relay_pieces(unit, range(SWAPPED, len(spans)))

                @pl.when(jnp.logical_and(c == 1, shared))
                def _():
                    for piece in range(SWAPPED, len(spans)):
                        span = pl.ds(*spans[piece])
                        arrived(x_recv.at[(unit - 3) // 2, piece - SWAPPED], ((spans[piece][1], width), 2))
                        remote(sbuf.at[unit, 1, span], sbuf.at[unit, 0, span], send_sem.at[SOURCE],
                               r_recv.at[unit - 2, 1], partner).start()

            with jax.named_scope("wait_relayed"):
                @pl.when(jnp.logical_not(shared))
                def _():
                    arrived(r_recv.at[unit - 2, 1], ((half // 2, width), 2))

                @pl.when(jnp.logical_and(c == 0, shared))
                def _():
                    arrived(r_recv.at[unit - 2, 1], ((half // 2 + swapped_rows, width), 2))

                @pl.when(jnp.logical_and(c == 1, shared))
                def _():
                    arrived(r_recv.at[unit - 2, 1], ((half // 2 - swapped_rows, width), 2))

            @pl.when(unit == units - 1)
            def _():
                project_half(unit, level, 1)

        @pl.when(index < (units - 1) * depth)
        def _():
            project(index)

    sent[SOURCE] += [source_part] * (units - 2 - (nx - 1))
    sent[SOURCE] += [((half - swapped_rows, width), 2)] * (nx - 1)

    def columns(parts):
        stacked = jnp.concatenate(parts, axis=0)
        fill = jnp.zeros((HEAD - stacked.shape[0], stacked.shape[1]), F32)
        return jnp.concatenate([stacked, fill], axis=0).T

    def weighted(cols, blocks, h):
        span = slice(h * HEAD, (h + 1) * HEAD)
        return sum(
            cols[0:piece_rows, k * heads + h:k * heads + h + 1] * block[:, span].astype(F32)
            for k, block in enumerate(blocks))

    def merge(layer, p):
        @pl.when(inner)
        def _():
            for slot, j in enumerate((far_edge, far_inner)):
                with jax.named_scope("merge_wait"):
                    arrived(m_recv.at[layer, p, slot], result_block, stats_block)
                with jax.named_scope("merge"):
                    mine, theirs = ssend[layer, p, j], srelay[layer, p, slot]
                    top = jnp.maximum(mine[0:heads], theirs[0:heads])
                    share = [jnp.exp2(one[0:heads] - top) for one in (mine, theirs)]
                    total = share[0] * mine[heads:] + share[1] * theirs[heads:]
                    cols = columns(share)
                    blocks = (osend[layer, p, j], orelay[layer, p, slot])
                    for h in range(heads):
                        osend[layer, p, j, :, h * HEAD:(h + 1) * HEAD] = weighted(
                            cols, blocks, h).astype(BF16)
                    ssend[layer, p, j] = jnp.concatenate([top, total], axis=0)
                    send_result(layer, p, j)

    def attend(layer, p, first, blocks, span, started=False):
        with jax.named_scope("attend"):
            count = blocks * piece_rows
            q = qbuf[layer, p, pl.ds(first, blocks)].reshape(count, local_width)
            lane = lax.broadcasted_iota(jnp.int32, (count, HEAD), 1)
            notes = jnp.zeros((count, HEAD), F32)
            ahead = head_scores(layer, q, 0, span)
            for h in range(heads):
                scores, peak = ahead
                if h + 1 < heads:
                    ahead = head_scores(layer, q, h + 1, span)
                cols = slice(h * HEAD, (h + 1) * HEAD)
                if started:
                    before = early_peak[p, :, cols]
                    peak = jnp.maximum(before, peak)
                    fade = jnp.exp2(before - peak)
                    shift = jnp.concatenate(
                        [peak] * (scores.shape[1] // HEAD), axis=1)
                    weights = jnp.exp2(scores * score_scale - shift)
                    total = jnp.sum(weights, axis=1, keepdims=True) + fade * early_total[p, :, cols]
                    o = jnp.dot(weights.astype(BF16), values[layer, span, cols], preferred_element_type=F32)
                    o = o + fade * early_sum[p, :, cols]
                else:
                    weights = jnp.exp2(scores * score_scale - peak)
                    total = jnp.sum(weights, axis=1, keepdims=True)
                    o = jnp.dot(weights.astype(BF16), values[layer, span, cols], preferred_element_type=F32)
                o = o.astype(BF16)
                for member in range(blocks):
                    osend[layer, p, first + member, :, cols] = o[member * piece_rows:(member + 1) * piece_rows]
                notes = jnp.where(lane == h, peak, notes)
                notes = jnp.where(lane == heads + h, total, notes)
            for two in range(blocks // 2):
                stats = notes[two * HEAD:(two + 1) * HEAD].T[0:2 * heads]
                ssend[layer, p, first + 2 * two] = stats
                ssend[layer, p, first + 2 * two + 1] = pltpu.roll(stats, piece_rows, 1)

    def keep_own(layer, p):
        orecv[layer, p, s] = osend[layer, p, s]
        srecv[layer, p, s] = ssend[layer, p, s]

    def out_project(layer, p):
        with jax.named_scope("wait_o"):
            arrived(o_recv.at[layer, p], *([result_block, stats_block] * 2))
        with jax.named_scope("combine_out"):
            origins = (s, near, far_inner)
            stats = [srecv[layer, p, j] for j in origins]
            top = functools.reduce(jnp.maximum, [one[0:heads] for one in stats])
            share = [jnp.exp2(one[0:heads] - top) for one in stats]
            total = sum(part * one[heads:] for part, one in zip(share, stats))
            cols = columns([part / total for part in share])
            blocks = [orecv[layer, p, j] for j in origins]
            for h in range(heads):
                attended[:, h * HEAD:(h + 1) * HEAD] = weighted(cols, blocks, h).astype(BF16)
            tile = min(512, width)
            for n in range(width // tile):
                span = slice(n * tile, (n + 1) * tile)
                part = jnp.dot(attended[...], wo[layer, :, span], preferred_element_type=F32).astype(BF16)
                for b in range(nx):
                    for core in range(CORES):
                        at = (b * CORES + core) * prows
                        pbuf[layer, p, core, b, :, span] = part[at:at + prows]
            go(remote(pbuf.at[layer, p, partner_c], half_in.at[layer, p], send_sem.at[ROW],
                      h_recv.at[layer, p], partner), ROW, chip_rows)

    def chip_total(layer, p):
        with jax.named_scope("chip_total"):
            arrived(h_recv.at[layer, p], chip_rows)
            for b in range(nx):
                both_cores = pbuf[layer, p, c, b].astype(F32) + half_in[layer, p, b].astype(F32)
                chip_sum[layer, p, x, c, b] = both_cores.astype(BF16)
            own = chip_sum.at[layer, p, x, c]
            for step in range(1, nx):
                go(remote(own, own, send_sem.at[ROW], c_recv.at[layer, p, nx - step - 1], peer(step)),
                   ROW, chip_rows)
            go(remote(own, own, send_sem.at[ROW], d_recv.at[layer, p], partner), ROW, chip_rows)

    def next_queries(layer, p):
        with jax.named_scope("xwait"):
            for step in range(1, nx):
                a = chip(step)
                other = chip_sum.at[layer, p, a, c]
                arrived(c_recv.at[layer, p, step - 1], chip_rows)
                go(remote(other, other, send_sem.at[ROW], d_recv.at[layer, p], partner), ROW, chip_rows)
            arrived(d_recv.at[layer, p], *([chip_rows] * nx))
        with jax.named_scope("norm_q"):
            for block in range(tp):
                projected = sum(
                    chip_sum[layer, p, a, block % CORES, block // CORES].astype(F32) for a in range(nx))
                value = stream[p, block] + normalize(projected, gains[layer, 1:2, :])
                stream[p, block] = value
                normed[p, block] = normalize(value, gains[layer + 1, 0:1, :]).astype(BF16)
            q = jnp.dot(normed[p].reshape(piece_rows, width), wq[layer + 1],
                        preferred_element_type=F32)
            qbuf[layer + 1, p, s] = q.astype(BF16)
            send_queries(layer + 1, p)

    def final_send(layer, p):
        with jax.named_scope("final_send"):
            arrived(h_recv.at[layer, p], chip_rows)
            for step in range(1, nx):
                b = chip(step)
                both_cores = pbuf[layer, p, c, b].astype(F32) + half_in[layer, p, b].astype(F32)
                fin[0, p, b] = both_cores.astype(BF16)
                go(remote(fin.at[0, p, b], fin.at[1, p, x], send_sem.at[ROW],
                          f_recv.at[p, nx - step - 1], peer(step)), ROW, sum_block)

    def final_rows(layer, p):
        with jax.named_scope("final_rows"):
            projected = pbuf[layer, p, c, x].astype(F32) + half_in[layer, p, x].astype(F32)
            for step in range(1, nx):
                b = chip(step)
                arrived(f_recv.at[p, step - 1], sum_block)
                projected = projected + fin[1, p, b].astype(F32)
            value = stream[p, t] + normalize(projected, gains[layer, 1:2, :])
            out[p * prows:(p + 1) * prows, :] = value.astype(out.dtype)

    for layer in range(depth):
        last = layer == depth - 1
        if layer > 0:
            hand_on(layer, 0)
        if layer == 1:
            @pl.loop(units * depth - (depth - 1), units * depth)
            def _(index):
                project(index)

        if layer == 0:
            @pl.loop(0, PIECES)
            def _(p):
                attend(layer, p, 2 * (1 - own_pair), 2, late, started=True)

                @pl.when(edge)
                def _():
                    send_aside(layer, p)

            @pl.loop(0, PIECES)
            def _(p):
                attend(layer, p, 2 * own_pair, 2, every)
                send_result(layer, p, near)
                keep_own(layer, p)
        else:
            @pl.loop(0, 2 * PIECES)
            def _(i):
                p = i // 2
                close = (i + jnp.where(jnp.logical_and(edge, p > 0), 1, 0)) % 2 == 0

                @pl.when(jnp.logical_and(i % 2 == 1, p + 1 < PIECES))
                def _():
                    hand_on(layer, p + 1)

                @pl.when(close)
                def _():
                    with jax.named_scope("wait_near"):
                        arrived(q_recv.at[layer - 1, p, near], result_block)

                @pl.when(jnp.logical_and(edge, jnp.logical_not(close)))
                def _():
                    with jax.named_scope("wait_far"):
                        for block in (far_inner, far_edge):
                            arrived(q_recv.at[layer - 1, p, block], result_block)

                attend(layer, p, jnp.where(close, 2 * own_pair, 2 * (1 - own_pair)), 2, every)

                @pl.when(close)
                def _():
                    keep_own(layer, p)

                @pl.when(jnp.logical_and(edge, close))
                def _():
                    send_result(layer, p, near)

                @pl.when(jnp.logical_and(inner, i == 2 * PIECES - 2))
                def _():
                    for later in range(PIECES):
                        send_result(layer, later, near)

                @pl.when(jnp.logical_and(edge, jnp.logical_not(close)))
                def _():
                    send_aside(layer, p)

        total = final_send if last else chip_total
        load(3, layer).wait()
        for p in range(PIECES):
            merge(layer, p)
        for p in range(PIECES):
            out_project(layer, p)
            total(layer, p)
        if not last:
            load(0, layer + 1).wait()
        for p in range(PIECES):
            if last:
                final_rows(layer, p)
            else:
                next_queries(layer, p)

    with jax.named_scope("finish"):
        drain_line()
        arrived(send_sem.at[ROW], *sent[ROW])
        moved = ((swapped_rows * (nx - 1), width), 2)

        @pl.when(c == 0)
        def _():
            arrived(send_sem.at[SOURCE], *sent[SOURCE])

        @pl.when(c == 1)
        def _():
            arrived(send_sem.at[SOURCE], *sent[SOURCE], moved, moved)


def fused_body(nx, sp, target, source, w_query, w_key, w_value, w_out, gains):
    depth, width, local_width = w_query.shape
    trows, rows = target.shape[0], source.shape[0]
    tp = nx * CORES
    prows = trows // PIECES
    piece_rows = tp * prows
    heads = local_width // HEAD
    units = 2 * nx
    vmem = pltpu.VMEM
    dma = pltpu.SemaphoreType.DMA
    anywhere = pl.BlockSpec(memory_space=pl.ANY)
    whole = pl.BlockSpec(memory_space=pltpu.VMEM)
    results = (depth, PIECES, sp, piece_rows, local_width)
    notes = (depth, PIECES, sp, 2 * heads, 2 * piece_rows)
    return pl.pallas_call(
        functools.partial(fused_kernel, nx, sp, depth),
        out_shape=jax.ShapeDtypeStruct((trows, width), BF16),
        in_specs=[anywhere] * 7,
        out_specs=whole,
        scratch_shapes=[
            vmem((tp, trows, width), BF16),
            vmem((units, 2, rows // 2, width), BF16),
            vmem(w_query.shape, BF16),
            vmem(w_key.shape, BF16),
            vmem(w_value.shape, BF16),
            vmem(w_out.shape, BF16),
            vmem((depth, units * rows, local_width), BF16),
            vmem((depth, units * rows, local_width), BF16),
            vmem((PIECES, tp, prows, width), F32),
            vmem((PIECES, tp, prows, width), BF16),
            vmem(results, BF16),
            vmem(results, BF16),
            vmem(results, BF16),
            vmem(notes, F32),
            vmem(notes, F32),
            vmem(results[:2] + (2,) + results[3:], BF16),
            vmem(notes[:2] + (2,) + notes[3:], F32),
            vmem((piece_rows, local_width), BF16),
            vmem((depth, PIECES, CORES, nx, prows, width), BF16),
            vmem((depth, PIECES, nx, prows, width), BF16),
            vmem((depth, PIECES, nx, CORES, nx, prows, width), BF16),
            vmem((2, PIECES, nx, prows, width), BF16),
            vmem((1024, 8, 128), F32),
            vmem(gains.shape, F32),
            vmem((PIECES, 2 * piece_rows, local_width), F32),
            vmem((PIECES, 2 * piece_rows, local_width), F32),
            vmem((PIECES, 2 * piece_rows, local_width), F32),
            dma((3,)), dma((3, depth)), dma((3,)), dma((nx,)),
            dma((units - 2, 4)), dma((1,)), dma((units - 2, 2)), dma((1,)), dma((depth - 1, PIECES, sp)),
            dma((nx - 1, 4 - SWAPPED)),
            dma((depth, PIECES)), dma((depth, PIECES, 2)), dma((depth, PIECES)),
            dma((depth - 1, PIECES, nx - 1)), dma((depth - 1, PIECES)), dma((PIECES, nx - 1)),
        ],
        compiler_params=pltpu.CompilerParams(
            collective_id=0, has_side_effects=True, vmem_limit_bytes=VMEM_KIB * 1024),
    )(*[pltpu.with_memory_space_constraint(one, pltpu.HBM) for one in (
        target, source, w_query, w_key, w_value, w_out, gains)])


def split_heads(row_block):
    return row_block.reshape(row_block.shape[0], row_block.shape[1] // HEAD, HEAD)


def body(target, source, w_query, w_key, w_value, w_out, gains):
    local_width = w_query.shape[2]
    score_scale = HEAD ** (-0.5)
    depth = w_query.shape[0]
    project_shard_part = lax.all_gather(source, "tp", axis=0, tiled=True)
    layer_parts = [
        jnp.stack(
            [
                jnp.dot(project_shard_part, w_key[level], preferred_element_type=jnp.float32),
                jnp.dot(project_shard_part, w_value[level], preferred_element_type=jnp.float32),
            ]
        )
        for level in range(depth)
    ]
    projected_source = jnp.stack(layer_parts).astype(jnp.bfloat16)
    stream = target.astype(jnp.float32)
    for layer_index in range(depth):
        normed = normalize(stream, gains[layer_index, 0]).astype(jnp.bfloat16)
        query_weight = w_query[layer_index]
        queries = jnp.dot(
            lax.all_gather(normed, "tp", axis=0, tiled=True),
            query_weight,
            preferred_element_type=jnp.float32,
        ).astype(jnp.bfloat16)
        row_count = queries.shape[0]
        keys_here = projected_source[layer_index, 0]
        values_here = projected_source[layer_index, 1]
        every_query = lax.all_gather(queries, "sp", axis=0, tiled=True)
        scores = (
            jnp.einsum(
                "qhd,khd->hqk",
                split_heads(every_query),
                split_heads(keys_here),
                preferred_element_type=jnp.float32,
            )
            * score_scale
        )
        row_peak = lax.pmax(jnp.max(scores, axis=2), "sp")
        weights = jnp.exp(scores - row_peak[:, :, None])
        local_summed = jnp.einsum(
            "hqk,khd->hqd",
            weights.astype(jnp.bfloat16),
            split_heads(values_here),
            preferred_element_type=jnp.float32,
        )
        summed, row_total = (
            lax.psum_scatter(
                local_summed.astype(jnp.bfloat16), "sp", scatter_dimension=1, tiled=True
            ).astype(jnp.float32),
            lax.psum_scatter(
                jnp.sum(weights, axis=2).astype(jnp.bfloat16), "sp", scatter_dimension=1, tiled=True
            ).astype(jnp.float32),
        )
        heads_out = summed / row_total[:, :, None]
        attended = (
            jnp.transpose(heads_out, (1, 0, 2)).reshape(row_count, local_width).astype(jnp.bfloat16)
        )
        out_weight = w_out[layer_index]
        projected = lax.psum_scatter(
            jnp.dot(attended, out_weight, preferred_element_type=jnp.float32).astype(jnp.bfloat16),
            "tp",
            scatter_dimension=0,
            tiled=True,
        ).astype(jnp.float32)
        stream = stream + normalize(projected, gains[layer_index, 1])
    return stream.astype(jnp.bfloat16)


def solution(mesh):
    in_specs = (
        P(("grp", "sp", "tp"), None),
        P(("grp", "sp", "tp"), None),
        P(None, None, "tp"),
        P(None, None, "tp"),
        P(None, None, "tp"),
        P(None, "tp", None),
        P(),
    )
    out_specs = P(("grp", "sp", "tp"), None)
    sp, tp = mesh.shape["sp"], mesh.shape["tp"]

    def run(target, source, w_query, w_key, w_value, w_out, gains):
        trows, rows, local_width = target.shape[0], source.shape[0], w_query.shape[2]
        tiles = (trows % (16 * PIECES) == 0 and tp * trows == PIECES * (HEAD // 2) and rows % 128 == 0
                 and sp % 2 == 0 and sp // 2 == 2 and w_query.shape[0] > 1 and tp > CORES
                 and local_width % (4 * HEAD) == 0 and tp % CORES == 0)
        form = functools.partial(fused_body, tp // CORES, sp) if tiles else body
        return form(target, source, w_query, w_key, w_value, w_out, gains)

    return jax.shard_map(run, mesh=mesh, in_specs=in_specs, out_specs=out_specs, check_vma=False)
```
